512 devices in a mesh: ep: 128 (over z, y, core), tp: 4 (over x).
Axes of the slice: x: 4, y: 8, z: 8, core: 2. Of those that a mesh axis runs over, the one named last changes fastest.
Arguments:
- tokens: bfloat16 [16384, 1024], P('ep'), may hold values from -6 to 6
- cotangent: bfloat16 [16384, 1024], P('ep'), may hold values from -1.5 to 1.5
- routing: int32 [16384, 2], P('ep'), may hold values from 0 to 31, all different within a row; in each aligned block of 128 rows (0 to 127, 128 to 255, ...) at most 12 rows name the same one
- gates: bfloat16 [16384, 2], P('ep'), may hold values from 0.099609375 to 0.8984375
- gate_proj: bfloat16 [128, 1024, 1024], P('ep', None, 'tp'), may hold values from -0.1875 to 0.1875
- up_proj: bfloat16 [128, 1024, 1024], P('ep', None, 'tp'), may hold values from -0.1875 to 0.1875
- down_proj: bfloat16 [128, 1024, 1024], P('ep', 'tp'), may hold values from -0.09375 to 0.09375
Outputs:
- token_grad: bfloat16 [16384, 1024], P('ep')
- gate_grad: float32 [16384, 2], P('ep')
- gate_proj_grad: bfloat16 [128, 1024, 1024], P('ep', None, 'tp')
- up_proj_grad: bfloat16 [128, 1024, 1024], P('ep', None, 'tp')
- down_proj_grad: bfloat16 [128, 1024, 1024], P('ep', 'tp')
- input_row_norms: float32 [32, 2, 1024], replicated
- hidden_row_norms: float32 [128, 1024], P('ep', 'tp')
The draws below stay inside these ranges and needn't reach their ends.
Inputs may be any that keep to these rules, and one draw needn't show every extreme that they name: `routing`: the two experts of a token differ. Among the 128 tokens of one ep index no expert is chosen more than 12 times, and on some ep index some expert is chosen exactly 12 times.
All inputs are finite; a program needn't handle non-finite values.
Results may differ from the reference program's by a relative error of at most 0.012.
Values may be sent and summed in bfloat16 or wider, within the bound.
No kernel may reach another device: no remote copies, remote signals or barrier semaphores. Data moves between devices by JAX's collectives and lax.ppermute only.
A program may use at most 128 MiB of HBM per device.

```python
import math
import jax
import jax.numpy as jnp
import numpy as np
from jax import lax

D = 1024
FF = 4096
TOP = 2
TOK_DEV = 128
TOKENS = 16384
EXPERTS = 32
SPAN = 4
FF_PART = 1024
FF_DEV = 256
SHARDS = 16
MOST = 12
N_EP = 128


def levels(stream_key, dims, pieces, least, top_value):
    def one(axis_at, blocks):
        draws = jax.random.uniform(jax.random.fold_in(jax.random.fold_in(stream_key, 6), axis_at), (blocks,), jnp.float32, least / len(pieces), top_value / len(pieces))
        return jnp.repeat(jnp.exp(draws), dims[axis_at] // blocks).reshape((-1,) + (1,) * (len(dims) - axis_at - 1))

    gain = one(*pieces[0])
    for cut in pieces[1:]:
        gain = gain * one(*cut)
    return gain


def assign_block(stream_key, own, number, rows, count, top, bound, slope):
    ranking = jax.random.permutation(stream_key, count)
    packed, common = shares(count, rows * top, bound, slope, True), shares(count, rows * top, bound, slope, False)
    places = jnp.arange(count)

    def named(lengths, turn):
        used = int((lengths > 0).sum())
        fixed = max(1, used // 4)
        moved = fixed + (places - fixed + turn * (used - fixed)) % max(1, count - fixed)
        return jnp.zeros((count,), jnp.int32).at[ranking[jnp.where(places < fixed, places, moved)]].set(jnp.asarray(lengths, jnp.int32))

    lengths = jnp.where(number % 4 == 0, named(packed, number // 4), named(common, number - number // 4 - 1))
    mixed = jax.random.permutation(jax.random.fold_in(own, 3), count)
    donor, receiver = mixed[0:count // 2 * 2:2], mixed[1:count // 2 * 2:2]
    margin = jnp.minimum(lengths[donor] - 1, bound - lengths[receiver]) // 2
    margin = jnp.where((donor == ranking[0]) | (receiver == ranking[0]) | (lengths[receiver] == 0), 0, jnp.maximum(margin, 0))
    moved = jax.random.randint(jax.random.fold_in(own, 4), (count // 2,), 0, 1 << 20) % (margin + 1)
    lengths = lengths.at[donor].add(-moved).at[receiver].add(moved)
    members = jnp.searchsorted(jnp.cumsum(lengths), jnp.arange(rows * top), side="right").astype(jnp.int32)
    table = members.reshape(top, rows).T
    table = table[jax.random.permutation(jax.random.fold_in(own, 1), rows)]
    turn = jax.random.randint(jax.random.fold_in(own, 2), (rows, 1), 0, top)
    return jnp.take_along_axis(table, (jnp.arange(top)[None, :] + turn) % top, axis=1)


def shares(count, total, reach, skew, full):
    weights = [(1 << 20) // math.isqrt(grade ** skew) + 1 for grade in range(1, count + 1)]
    largest = reach if full else min(reach, max(-(-total // count), total * weights[0] // sum(weights)))
    least = 1 if total - largest >= count - 1 else 0
    counts, surplus = [largest] + [least] * (count - 1), total - largest - least * (count - 1)
    while surplus > 0:
        movable = [i for i in range(1, count) if counts[i] < largest] or [i for i in range(1, count) if counts[i] < reach]
        pool, budget = sum([weights[i] for i in movable]), surplus
        for i in movable:
            extra = min(reach - counts[i], max(1, budget * weights[i] // pool), surplus)
            counts[i] = counts[i] + extra
            surplus = surplus - extra
    return np.array(counts)


def bell_draw(rng, extent, width, reach, shards=(), kind=jnp.bfloat16):
    entries = width * jax.random.normal(rng, extent, jnp.float32)
    if shards:
        entries = entries * levels(rng, extent, shards, -0.22, 0.18)
    return jnp.clip(entries, -reach, reach).astype(kind)


def setup_inputs(seed: int = 0) -> dict:
    streams_of = jax.random.split(jax.random.key(seed), 8)
    tokens = bell_draw(streams_of[0], (TOKENS, D), 1.0, 6.0, ((0, 128),))
    cotangent = bell_draw(streams_of[1], (TOKENS, D), 0.25, 1.5, ((0, 128),))
    routing_keys = jax.random.split(jax.random.fold_in(streams_of[2], 1), TOKENS // TOK_DEV)
    routing_turns = jax.random.permutation(jax.random.fold_in(streams_of[2], 3), TOKENS // TOK_DEV)
    routing = jax.vmap(lambda own, number: assign_block(jax.random.fold_in(streams_of[2], 2), own, number, TOK_DEV, EXPERTS, TOP, MOST, 2))(routing_keys, routing_turns).reshape((TOKENS, TOP))
    gates = jnp.clip(0.099609375 + 0.7988281 * jax.random.uniform(streams_of[3], (TOKENS, TOP), jnp.float32) ** levels(streams_of[3], (TOKENS, TOP), ((0, 128),), -0.2, 0.2), 0.099609375, 0.8984375).astype(jnp.bfloat16)
    gate_proj = bell_draw(streams_of[4], (N_EP, D, FF_PART), D ** -0.5, 0.1875, ((0, 128), (2, 4)))
    up_proj = bell_draw(streams_of[5], (N_EP, D, FF_PART), D ** -0.5, 0.1875, ((0, 128), (2, 4)))
    down_proj = bell_draw(streams_of[6], (N_EP, FF_PART, D), FF ** -0.5, 0.09375, ((0, 128), (1, 4)))
    return {"tokens": tokens, "cotangent": cotangent, "routing": routing, "gates": gates, "gate_proj": gate_proj, "up_proj": up_proj, "down_proj": down_proj}


def expert_backward(rows_x, rows_dy, rows_g, w_gate, w_up, w_down):
    pre_gate = jnp.dot(rows_x, w_gate, preferred_element_type=jnp.float32)
    pre_up = jnp.dot(rows_x, w_up, preferred_element_type=jnp.float32)
    sigmoid_gate = jax.nn.sigmoid(pre_gate)
    activated = pre_gate * sigmoid_gate
    hidden_back = lax.dot_general(rows_dy, w_down, (((1,), (1,)), ((), ())), preferred_element_type=jnp.float32)
    gate_val = rows_g.astype(jnp.float32)[:, None]
    scaled = (gate_val * activated * pre_up).astype(jnp.bfloat16)
    hid_grad = gate_val * hidden_back
    grad_gate_pre = (hid_grad * pre_up * sigmoid_gate * (1.0 + pre_gate * (1.0 - sigmoid_gate))).astype(jnp.bfloat16)
    grad_up_pre = (hid_grad * activated).astype(jnp.bfloat16)
    down_grad = lax.dot_general(scaled, rows_dy, (((0,), (0,)), ((), ())), preferred_element_type=jnp.float32)
    gate_grad_w = lax.dot_general(rows_x, grad_gate_pre, (((0,), (0,)), ((), ())), preferred_element_type=jnp.float32)
    up_grad_w = lax.dot_general(rows_x, grad_up_pre, (((0,), (0,)), ((), ())), preferred_element_type=jnp.float32)
    products = hidden_back * activated * pre_up
    return products, grad_gate_pre, grad_up_pre, down_grad, gate_grad_w, up_grad_w


def reference(tokens, cotangent, routing, gates, gate_proj, up_proj, down_proj):
    pair_expert = routing.reshape(N_EP, TOK_DEV * TOP).astype(jnp.int32)
    onehot = (pair_expert[:, :, None] == jnp.arange(EXPERTS, dtype=jnp.int32)[None, None, :]).astype(jnp.int32)
    before = jnp.cumsum(onehot, axis=1) - onehot
    slot_rank = jnp.sum(before * onehot, axis=2).astype(jnp.int32)
    pair_index = jnp.arange(TOKENS * TOP, dtype=jnp.int32).reshape(N_EP, TOK_DEV * TOP)
    source = jnp.broadcast_to(jnp.arange(N_EP, dtype=jnp.int32)[:, None], pair_expert.shape)
    slot_table = jnp.full((EXPERTS, N_EP, MOST), TOKENS * TOP, jnp.int32)
    slot_table = slot_table.at[pair_expert, source, slot_rank].set(pair_index)
    tokens_ext = jnp.concatenate([tokens, jnp.zeros((1, D), jnp.bfloat16)], axis=0)
    cot_ext = jnp.concatenate([cotangent, jnp.zeros((1, D), jnp.bfloat16)], axis=0)
    gates_ext = jnp.concatenate([gates.reshape(-1), jnp.zeros((1,), jnp.bfloat16)], axis=0)
    gate_w = gate_proj.reshape(EXPERTS, SPAN, D, FF_PART).transpose(0, 2, 1, 3).reshape(EXPERTS, D, FF)
    up_w = up_proj.reshape(EXPERTS, SPAN, D, FF_PART).transpose(0, 2, 1, 3).reshape(EXPERTS, D, FF)
    down_w = down_proj.reshape(EXPERTS, FF, D)

    def one_expert(operands):
        slot_index, w_gate, w_up, w_down = operands
        chosen = slot_index.reshape(-1)
        token_row = (chosen // TOP).astype(jnp.int32)
        rows_x = tokens_ext[token_row]
        rows_dy = cot_ext[token_row]
        rows_g = gates_ext[chosen]
        products, grad_gate_pre, grad_up_pre, down_grad, gate_grad_w, up_grad_w = expert_backward(
            rows_x, rows_dy, rows_g, w_gate, w_up, w_down)
        row_count = chosen.shape[0]
        gate_blocks = jnp.sum(products.reshape(row_count, SHARDS, FF_DEV), axis=2).astype(jnp.bfloat16)
        gate_blocks = lax.optimization_barrier(gate_blocks)
        gate_sum = jnp.sum(gate_blocks.astype(jnp.float32), axis=1)
        gate_cols = grad_gate_pre.reshape(row_count, SHARDS, FF_DEV).astype(jnp.float32)
        up_cols = grad_up_pre.reshape(row_count, SHARDS, FF_DEV).astype(jnp.float32)
        wg_blocks = w_gate.reshape(D, SHARDS, FF_DEV).astype(jnp.float32)
        wu_blocks = w_up.reshape(D, SHARDS, FF_DEV).astype(jnp.float32)
        block_rows = jnp.einsum('rqf,dqf->rqd', gate_cols, wg_blocks) + jnp.einsum('rqf,dqf->rqd', up_cols, wu_blocks)
        block_rows = lax.optimization_barrier(block_rows.astype(jnp.bfloat16))
        row_grad = jnp.sum(block_rows.astype(jnp.float32), axis=1)
        in_norms = jnp.stack([jnp.sum(gate_grad_w * gate_grad_w, axis=1), jnp.sum(up_grad_w * up_grad_w, axis=1)])
        hid_norms = jnp.sum(down_grad * down_grad, axis=1)
        return (chosen, row_grad, gate_sum, gate_grad_w.astype(jnp.bfloat16), up_grad_w.astype(jnp.bfloat16),
                down_grad.astype(jnp.bfloat16), in_norms, hid_norms)

    chosen, row_grad, gate_sum, gate_grads, up_grads, down_grads, in_norms, hid_norms = lax.map(
        one_expert, (slot_table, gate_w, up_w, down_w))
    flat_chosen = chosen.reshape(-1)
    token_acc = jnp.zeros((TOKENS + 1, D), jnp.float32).at[(flat_chosen // TOP).astype(jnp.int32)].add(row_grad.reshape(-1, D))
    token_grad = token_acc[:TOKENS].astype(jnp.bfloat16)
    gate_acc = jnp.zeros((TOKENS * TOP + 1,), jnp.float32).at[flat_chosen].add(gate_sum.reshape(-1))
    gate_grad = gate_acc[:TOKENS * TOP].reshape(TOKENS, TOP)
    gate_proj_grad = gate_grads.reshape(EXPERTS, D, SPAN, FF_PART).transpose(0, 2, 1, 3).reshape(N_EP, D, FF_PART)
    up_proj_grad = up_grads.reshape(EXPERTS, D, SPAN, FF_PART).transpose(0, 2, 1, 3).reshape(N_EP, D, FF_PART)
    down_proj_grad = down_grads.reshape(N_EP, FF_PART, D)
    hidden_row_norms = hid_norms.reshape(N_EP, FF_PART)
    return (token_grad, gate_grad, gate_proj_grad, up_proj_grad, down_proj_grad, in_norms, hidden_row_norms)
```

```python
import jax
import jax.numpy as jnp
import numpy as np
from jax import lax
from jax.experimental import pallas as pl
from jax.experimental.pallas import tpu as pltpu
from jax.sharding import Mesh
from jax.sharding import PartitionSpec as P

EP = ("z", "yh", "yp", "c")
HOMES = ("z", "yh")
GROUP = ("yp", "tp")
BF = jnp.bfloat16
F32 = jnp.float32
T, D, H = 128, 1024, 256
EXPERTS, SLOTS, SRC = 32, 12, 32
ROWS = SRC * SLOTS
CH = 192
ALL = 2 * ROWS
SENT = 2 * ROWS + SRC
TURNS = (0, 3, 1, 2)
NN = (((1,), (0,)), ((), ()))
NT = (((1,), (1,)), ((), ()))
TN = (((0,), (0,)), ((), ()))


def dot(a, b, dims=NN):
    return lax.dot_general(a, b, dims, preferred_element_type=F32)


def iota(shape, dim):
    return lax.broadcasted_iota(jnp.int32, shape, dim)


def call(kernel, outs, scalars, *args):
    specs = [pl.BlockSpec(memory_space=pltpu.SMEM)] if scalars is not None else []
    args = ([scalars] if scalars is not None else []) + list(args)
    specs = specs + [pl.BlockSpec(memory_space=pltpu.VMEM) for _ in range(len(args) - len(specs))]
    return kernel(outs, specs)(*args)


def kernel_of(body, name, scratch=(), flops=2**27):
    def build(outs, specs):
        return pl.pallas_call(
            body,
            out_shape=outs,
            in_specs=specs,
            out_specs=jax.tree.map(lambda _: pl.BlockSpec(memory_space=pltpu.VMEM), outs),
            scratch_shapes=list(scratch),
            compiler_params=pltpu.CompilerParams(vmem_limit_bytes=56 * 1024 * 1024),
            cost_estimate=pl.CostEstimate(flops=flops, transcendentals=0, bytes_accessed=2**20),
            name=name,
        )

    return build


def shape(dims, dtype=BF):
    return jax.ShapeDtypeStruct(dims, dtype)


def tables():
    o = np.arange(192)
    regroup = (o % 48 // 12 * 48 + o // 48 * 12 + o % 12)[:, None] == np.arange(192)[None, :]
    r = np.arange(CH)
    lane = (r % SLOTS)[:, None] == np.arange(128)[None, :]
    source = np.arange(16)[:, None] == (r // SLOTS)[None, :]
    j = np.arange(256)
    src, row = j // 32, j % 32
    at = np.where(row < 24, row // 12 * 96 + src * 12 + row % 12, 200 + row - 25)
    at = np.where(row == 24, 192 + src, at)
    back = (at[:, None] == np.arange(208)[None, :]) & (row < 29)[:, None]
    return tuple(jnp.asarray(a.astype(np.float32), BF) for a in (regroup, lane, source, back))


def dispatch_body(at, rt, gt, tok, cot, out):
    x = at[0]
    r0, r1 = rt[0:1, :], rt[1:2, :]
    g0, g1 = gt[0:1, :].astype(F32), gt[1:2, :].astype(F32)
    e = iota((EXPERTS, T), 0)
    m0, m1 = (e == r0).astype(F32), (e == r1).astype(F32)
    earlier = (iota((T, T), 0) < iota((T, T), 1)).astype(F32).astype(BF)
    before = dot((m0 + m1).astype(BF), earlier)
    base0 = r0 * 48 + jnp.sum(m0 * before, axis=0, keepdims=True).astype(jnp.int32)
    base1 = r1 * 48 + jnp.sum(m1 * before, axis=0, keepdims=True).astype(jnp.int32)

    def step(i, carry):
        row = iota((192, T), 0) + i * 192
        total = jnp.zeros((192, 128), F32)
        for half in range(2):
            cols = pl.ds(pl.multiple_of((x * 2 + half) * 128, 128), 128)
            for kind in range(2):
                off = kind * 24 + half * 12
                hit0, hit1 = row == base0 + off, row == base1 + off
                if kind == 0:
                    pick = jnp.where(hit0 | hit1, 1.0, 0.0)
                    total += dot(pick.astype(BF), tok[:, cols])
                else:
                    pick = jnp.where(hit0, g0, jnp.where(hit1, g1, 0.0))
                    total += dot(pick.astype(BF), cot[:, cols])
        out[pl.ds(pl.multiple_of(i * 192, 192), 192), :] = total.astype(BF)
        return carry

    lax.fori_loop(0, 8, step, 0)


def regroup_body(order, rows, out):
    for b in range(8):
        moved = dot(order[...], rows[b * 192 : (b + 1) * 192, :]).astype(BF)
        for k in range(4):
            out[k * ROWS + b * 48 : k * ROWS + (b + 1) * 48, :] = moved[k * 48 : (k + 1) * 48]


def places(at):
    return [pl.ds(pl.multiple_of(lax.rem(at[0] + turn, 4) * H, H), H) for turn in TURNS]


def rows_of(pieces, kind, first, count):
    cols = []
    for piece in pieces:
        for half in range(2):
            start = (kind * 2 + half) * ROWS + first
            cols.append(piece[pl.ds(start, count), :])
    return jnp.concatenate(cols, axis=1)


def expert_body(at, lane, source, *refs):
    pieces, (wg, wgo, wu, wuo, wd, wdo) = refs[:8], refs[8:14]
    out, scaled_o, ggp_o, gup_o = refs[14:18]
    pg, pu, pd = refs[18:21]
    half = at[1]
    for t, here in enumerate(places(at)):
        there = slice(t * H, (t + 1) * H)
        for mat, mine, other in ((pg, wg, wgo), (pu, wu, wuo)):
            mat[there, :H] = mine[here, :]
            mat[there, H:] = other[here, :]
        pd[:H, there] = wd[:, here]
        pd[H:, there] = wdo[:, here]
    for group in range(2):
        parity = half if group == 0 else 1 - half

        def step(i, carry, group=group, parity=parity):
            first = pl.multiple_of(i * CH, CH)
            kept = pl.ds(pl.multiple_of(group * ROWS + i * CH, CH), CH)
            rows_x = rows_of(pieces[group::2], 0, first, CH)
            rows_y = rows_of(pieces[group::2], 1, first, CH)
            pre_gate = dot(rows_x, pg[...])
            pre_up = dot(rows_x, pu[...])
            back = dot(rows_y, pd[...], NT)
            s = jax.nn.sigmoid(pre_gate)
            act = pre_gate * s
            prod = act * pre_up
            scaled_o[kept, :] = prod.astype(BF)
            ggp = (back * pre_up * s * (1.0 + pre_gate * (1.0 - s))).astype(BF)
            gup = (back * act).astype(BF)
            ggp_o[kept, :] = ggp
            gup_o[kept, :] = gup
            part = jnp.sum(back * prod, axis=1, keepdims=True)
            spread = (part * lane[...].astype(F32)).astype(BF)
            gates = dot(source[...], spread).astype(BF)
            grad = dot(ggp[:, :H], wg[...], NT) + dot(ggp[:, H:], wgo[...], NT)
            grad += dot(gup[:, :H], wu[...], NT) + dot(gup[:, H:], wuo[...], NT)
            grad = grad.astype(BF)
            for x in range(4):
                there = parity * 4 + x
                for b in range(2):
                    cols = slice((x * 2 + b) * 128, (x * 2 + b + 1) * 128)
                    out[there, pl.ds(b * ROWS + first, CH), :] = grad[:, cols]
                out[there, pl.ds(pl.multiple_of(ALL + i * 16, 16), 16), :] = gates
            return carry

        lax.fori_loop(0, ROWS // CH, step, 0)


def weights_body(at, *refs):
    pieces, (scaled, ggp, gup) = refs[:8], refs[8:11]
    g_own, u_own, d_own, far = refs[11:15]
    for t, here in enumerate(places(at)):
        both = [[rows_of((pieces[2 * t + n],), kind, 0, ROWS) for n in range(2)] for kind in range(2)]
        rows_x, rows_y = (jnp.concatenate(b, axis=0) for b in both)
        for n, own, left in ((0, g_own, ggp), (1, u_own, gup)):
            grad = dot(rows_x, left[...], TN)
            own[here, :] = grad[:, :H]
            far[n, here, :] = grad[:, H:].astype(BF)
        down = dot(scaled[...], rows_y, TN)
        d_own[:, here] = down[:H]
        far[2, here, :] = down[H:].astype(BF)


def sums_body(g_own, u_own, d_own, far, g_out, u_out, d_out, in_sq, hid_sq):
    ones = jnp.ones((8, H), BF)
    in_sq[...] = jnp.zeros((16, 8, 128), F32)
    for k, (own, out) in enumerate(((g_own, g_out), (u_own, u_out))):
        grad = own[...] + far[k].astype(F32)
        out[...] = grad.astype(BF)
        squares = dot(ones, (grad * grad).astype(BF), NT)
        for b in range(8):
            row = k * 2 + b % 2
            for copy in range(4):
                in_sq[copy * 4 + b // 2, row : row + 1, :] = squares[0:1, b * 128 : (b + 1) * 128]
    total = jnp.zeros((8, H), F32)
    for b in range(4):
        cols = slice(b * H, (b + 1) * H)
        grad = d_own[:, cols] + far[2, cols, :].astype(F32)
        d_out[:, cols] = grad.astype(BF)
        total += dot(ones, (grad * grad).astype(BF), NT)
    hid_sq[...] = total[0:1]


def back_body(order, parts, squares, out):
    norms = jnp.sum(squares[...], axis=0)

    def total(first, count):
        rows = slice(first, first + count)
        added = parts[0, rows, :].astype(F32)
        for k in range(1, 8):
            added += parts[k, rows, :].astype(F32)
        return added

    gates = total(ALL, SRC)
    for b in range(4):
        filled = [total(b * 96, 96), total(ROWS + b * 96, 96), gates[b * 8 : (b + 1) * 8], norms]
        filled = jnp.concatenate(filled, axis=0).astype(BF)
        out[b * 256 : (b + 1) * 256, :] = dot(order[...], filled).astype(BF)


def combine_body(rt, gt, got, out, gate):
    diagonal = iota((T, T), 0) == iota((T, T), 1)

    def column(row):
        return jnp.sum(jnp.where(diagonal, row, 0.0), axis=1, keepdims=True)

    r0, r1 = (column(rt[k : k + 1, :].astype(F32)).astype(jnp.int32) for k in range(2))
    gates = [column(gt[k : k + 1, :].astype(F32)) for k in range(2)]
    e = iota((T, 128), 1)
    m0, m1 = (e == r0).astype(F32), (e == r1).astype(F32)
    earlier = (iota((T, T), 1) < iota((T, T), 0)).astype(F32).astype(BF)
    before = dot(earlier, (m0 + m1).astype(BF))
    rank0 = jnp.sum(m0 * before, axis=1, keepdims=True).astype(jnp.int32)
    rank1 = jnp.sum(m1 * before, axis=1, keepdims=True).astype(jnp.int32)
    row = iota((T, 1024), 1)
    rows = got[...]
    for half in range(2):
        hit0 = row == r0 * 32 + rank0 + half * 12
        hit1 = row == r1 * 32 + rank1 + half * 12
        pick = jnp.where(hit0 | hit1, 1.0, 0.0).astype(BF)
        out[half * T : (half + 1) * T, :] = dot(pick, rows).astype(BF)
    for k, (r, rank) in enumerate(((r0, rank0), (r1, rank1))):
        both = dot(jnp.where(row == r * 32 + 24, 1.0, 0.0).astype(BF), rows)
        total = jnp.sum(jnp.where(e == rank, both, 0.0), axis=1, keepdims=True)
        share = jnp.where(diagonal, total / gates[k], 0.0)
        gate[k : k + 1, :] = jnp.sum(share, axis=0, keepdims=True)
    n = iota((T, 1024), 0)
    hit = row == (n & 31) * 32 + 25 + ((n >> 5) & 1) * 2 + (n >> 6)
    out[2 * T :, :] = dot(jnp.where(hit, 1.0, 0.0).astype(BF), rows).astype(BF)


def final_body(got, token, norms):
    for x in range(4):
        for half in range(2):
            cols = slice((x * 2 + half) * 128, (x * 2 + half + 1) * 128)
            token[:, cols] = got[x * 384 + half * T : x * 384 + (half + 1) * T, :]
            first = x * 384 + 2 * T + half * 64
            for kind in range(2):
                rows = got[first + kind * 32 : first + kind * 32 + 32, :]
                norms[:, kind, cols] = rows.astype(F32)


SWAP = [(0, 1), (1, 0)]


def turned(x, by):
    return lax.ppermute(x, "tp", [(i, (i + by) % 4) for i in range(4)])


def body(tokens, cotangent, routing, gates, gate_proj, up_proj, down_proj):
    regroup, lane, source, back = tables()
    at = jnp.stack([lax.axis_index("tp"), lax.axis_index("yp")]).astype(jnp.int32)
    weights = (gate_proj[0], up_proj[0], down_proj[0])
    sent = call(
        kernel_of(dispatch_body, "dispatch"), shape((1536, 128)), at,
        routing.T, gates.T, tokens, cotangent,
    )
    others = [lax.ppermute(w, "c", SWAP) for w in weights]
    moved = lax.all_to_all(sent.reshape(SRC, 48, 128), HOMES, 0, 0, tiled=True)
    mine = call(
        kernel_of(regroup_body, "regroup"), shape((1536, 128)), None,
        regroup, moved.reshape(1536, 128),
    )
    mine2 = turned(mine, 2)
    near = lax.ppermute(mine, "yp", SWAP)
    mine1, mine3 = turned(mine, 1), turned(mine, -1)
    near2 = lax.ppermute(mine2, "yp", SWAP)
    near1, near3 = turned(near, 1), turned(near, -1)
    pieces = (mine, near, mine1, near1, mine3, near3, mine2, near2)
    ordered = [w for pair in zip(weights, others) for w in pair]
    hidden = shape((ALL, 2 * H))
    rows, scaled, ggp, gup = call(
        kernel_of(
            expert_body, "expert",
            [pltpu.VMEM((D, 2 * H), BF), pltpu.VMEM((D, 2 * H), BF), pltpu.VMEM((2 * H, D), BF)],
            flops=2**32,
        ),
        (shape((8, SENT, 128)), hidden, hidden, hidden), at,
        lane, source, *pieces, *ordered,
    )
    parts = lax.all_to_all(rows, GROUP, 0, 0, tiled=True)
    g_own, u_own, d_own, far = call(
        kernel_of(weights_body, "weights", flops=2**31),
        (shape((D, H), F32), shape((D, H), F32), shape((H, D), F32), shape((3, D, H))),
        at, *pieces, scaled, ggp, gup,
    )
    far = lax.ppermute(far, "c", SWAP)
    gate_grad, up_grad, down_grad, squares, hid_sq = call(
        kernel_of(sums_body, "sums", flops=2**29),
        (
            shape((D, H)), shape((D, H)), shape((H, D)),
            shape((16, 8, 128), F32), shape((1, H), F32),
        ),
        None, g_own, u_own, d_own, far,
    )
    squares, parts = lax.optimization_barrier((squares, parts))
    squares = lax.all_to_all(squares, ("c",) + GROUP, 0, 0, tiled=True)
    answer = call(kernel_of(back_body, "back"), shape((1024, 128)), None, back, parts, squares)
    got = lax.all_to_all(answer.reshape(SRC, 32, 128), HOMES, 0, 0, tiled=True)
    own, gate = call(
        kernel_of(combine_body, "combine"), (shape((384, 128)), shape((2, T), F32)), None,
        routing.T, gates.T, got.reshape(1024, 128),
    )
    every = lax.all_gather(own, "tp", axis=0, tiled=True)
    token, norms = call(
        kernel_of(final_body, "final"), (shape((T, D)), shape((EXPERTS, 2, D), F32)), None, every
    )
    return (
        token,
        gate.T,
        gate_grad[None],
        up_grad[None],
        down_grad[None],
        norms,
        hid_sq,
    )


def solution(mesh):
    devices = mesh.devices.reshape(8, 4, 2, 2, mesh.shape["tp"])
    split = Mesh(devices, ("z", "yh", "yp", "c", "tp"))
    placed = (
        P(EP, None), P(EP, None), P(EP, None), P(EP, None),
        P(EP, None, "tp"), P(EP, None, "tp"), P(EP, "tp", None),
    )
    return jax.shard_map(
        body,
        mesh=split,
        in_specs=placed,
        out_specs=(
            P(EP, None), P(EP, None), P(EP, None, "tp"), P(EP, None, "tp"), P(EP, "tp", None),
            P(), P(EP, "tp"),
        ),
        check_vma=False,
    )
```

```python
import jax
import jax.numpy as jnp
import numpy as np
from jax import lax
from jax.experimental import pallas as pl
from jax.experimental.pallas import tpu as pltpu
from jax.sharding import Mesh
from jax.sharding import PartitionSpec as P

EP = ("z", "yh", "yp", "c")
HOMES = ("z", "yh")
GROUP = ("yp", "tp")
BF = jnp.bfloat16
F32 = jnp.float32
T, D, H = 128, 1024, 256
EXPERTS, SLOTS, SRC = 32, 12, 32
ROWS = SRC * SLOTS
CH = 192
ALL = 2 * ROWS
SENT = 2 * ROWS + SRC
VM = (8, 8, 8)
TURNS = (0, 3, 1, 2)
NN = (((1,), (0,)), ((), ()))
NT = (((1,), (1,)), ((), ()))
TN = (((0,), (0,)), ((), ()))


def dot(a, b, dims=NN):
    return lax.dot_general(a, b, dims, preferred_element_type=F32)


def iota(shape, dim):
    return lax.broadcasted_iota(jnp.int32, shape, dim)


def call(kernel, outs, *args):
    return kernel(outs, [pl.BlockSpec(memory_space=pltpu.VMEM) for _ in args])(*args)


def kernel_of(body, name, flops=2**27, vmem=4):
    def build(outs, specs):
        return pl.pallas_call(
            body,
            out_shape=outs,
            in_specs=specs,
            out_specs=jax.tree.map(lambda _: pl.BlockSpec(memory_space=pltpu.VMEM), outs),
            compiler_params=pltpu.CompilerParams(vmem_limit_bytes=vmem * 1024 * 1024),
            cost_estimate=pl.CostEstimate(flops=flops, transcendentals=0, bytes_accessed=2**20),
            name=name,
        )

    return build


def shape(dims, dtype=BF):
    return jax.ShapeDtypeStruct(dims, dtype)


def tables():
    o = np.arange(192)
    regroup = (o % 48 // 12 * 48 + o // 48 * 12 + o % 12)[:, None] == np.arange(192)[None, :]
    r = np.arange(CH)
    lane = (r % SLOTS)[:, None] == np.arange(128)[None, :]
    source = np.arange(16)[:, None] == (r // SLOTS)[None, :]
    j = np.arange(256)
    src, row = j // 32, j % 32
    at = np.where(row < 24, row // 12 * 96 + src * 12 + row % 12, 200 + row - 25)
    at = np.where(row == 24, 192 + src, at)
    back = (at[:, None] == np.arange(208)[None, :]) & (row < 29)[:, None]
    return tuple(jnp.asarray(a.astype(np.float32), BF) for a in (regroup, lane, source, back))


def dispatch_body(rt, gt, tok, cot, out):
    x = lax.axis_index("tp")
    r0, r1 = rt[0:1, :], rt[1:2, :]
    g0, g1 = gt[0:1, :].astype(F32), gt[1:2, :].astype(F32)
    e = iota((EXPERTS, T), 0)
    m0, m1 = (e == r0).astype(F32), (e == r1).astype(F32)
    earlier = (iota((T, T), 0) < iota((T, T), 1)).astype(F32).astype(BF)
    before = dot((m0 + m1).astype(BF), earlier)
    base0 = r0 * 48 + jnp.sum(m0 * before, axis=0, keepdims=True).astype(jnp.int32)
    base1 = r1 * 48 + jnp.sum(m1 * before, axis=0, keepdims=True).astype(jnp.int32)

    def step(i, carry):
        row = iota((192, T), 0) + i * 192
        total = jnp.zeros((192, 128), F32)
        for half in range(2):
            cols = pl.ds(pl.multiple_of((x * 2 + half) * 128, 128), 128)
            for kind in range(2):
                off = kind * 24 + half * 12
                hit0, hit1 = row == base0 + off, row == base1 + off
                if kind == 0:
                    pick = jnp.where(hit0 | hit1, 1.0, 0.0)
                    total += dot(pick.astype(BF), tok[:, cols])
                else:
                    pick = jnp.where(hit0, g0, jnp.where(hit1, g1, 0.0))
                    total += dot(pick.astype(BF), cot[:, cols])
        out[pl.ds(pl.multiple_of(i * 192, 192), 192), :] = total.astype(BF)
        return carry

    lax.fori_loop(0, 8, step, 0)


def regroup_body(order, rows, out):
    for b in range(8):
        moved = dot(order[...], rows[b * 192 : (b + 1) * 192, :]).astype(BF)
        for k in range(4):
            out[k * ROWS + b * 48 : k * ROWS + (b + 1) * 48, :] = moved[k * 48 : (k + 1) * 48]


def blocks():
    x = lax.axis_index("tp")
    return [lax.rem(x + turn, 4) for turn in TURNS]


def places():
    return [pl.ds(pl.multiple_of(b * H, H), H) for b in blocks()]


def prepare_body(wg, wgo, wu, wuo, wd, wdo, pg, pu, pd):
    for t, here in enumerate(places()):
        there = slice(t * H, (t + 1) * H)
        for mat, mine, other in ((pg, wg, wgo), (pu, wu, wuo)):
            mat[there, :H] = mine[here, :]
            mat[there, H:] = other[here, :]
        pd[:H, there] = wd[:, here]
        pd[H:, there] = wdo[:, here]


def rows_of(pieces, kind, first, count):
    cols = []
    for piece in pieces:
        for half in range(2):
            start = (kind * 2 + half) * ROWS + first
            cols.append(piece[pl.ds(start, count), :])
    return jnp.concatenate(cols, axis=1)


def expert_rows(pieces, lane, source, pg, pu, pd, out, group, scaled_o, ggp_o, gup_o):
    def step(i, carry):
        first = pl.multiple_of(i * CH, CH)
        kept = pl.ds(first, CH)
        rows_x = rows_of(pieces, 0, first, CH)
        rows_y = rows_of(pieces, 1, first, CH)
        pre_gate = dot(rows_x, pg[...])
        pre_up = dot(rows_x, pu[...])
        back = dot(rows_y, pd[...], NT)
        s = jax.nn.sigmoid(pre_gate)
        act = pre_gate * s
        prod = act * pre_up
        scaled_o[kept, :] = prod.astype(BF)
        ggp = (back * pre_up * s * (1.0 + pre_gate * (1.0 - s))).astype(BF)
        gup = (back * act).astype(BF)
        ggp_o[kept, :] = ggp
        gup_o[kept, :] = gup
        part = jnp.sum(back * prod, axis=1, keepdims=True)
        spread = (part * lane[...].astype(F32)).astype(BF)
        gates = dot(source[...], spread).astype(BF)
        grad = (dot(ggp, pg[...], NT) + dot(gup, pu[...], NT)).astype(BF)
        for t, x in enumerate(blocks()):
            for b in range(2):
                cols = slice((t * 2 + b) * 128, (t * 2 + b + 1) * 128)
                out[group * 4 + x, pl.ds(b * ROWS + first, CH), :] = grad[:, cols]
            out[group * 4 + x, pl.ds(pl.multiple_of(ALL + i * 16, 16), 16), :] = gates
        return carry

    lax.fori_loop(0, ROWS // CH, step, 0)


def first_body(lane, source, *refs):
    pieces, (pg, pu, pd), (out, *hidden) = refs[:4], refs[4:7], refs[7:]
    expert_rows(pieces, lane, source, pg, pu, pd, out, 0, *hidden)


def second_body(lane, source, early, *refs):
    pieces, (pg, pu, pd), (out, *hidden) = refs[:4], refs[4:7], refs[7:]
    half = lax.axis_index("yp")
    for x in range(4):
        out[half * 4 + x] = early[x]
    expert_rows(pieces, lane, source, pg, pu, pd, out, 1 - half, *hidden)


def weights_body(*refs):
    pieces = refs[:4], refs[4:8]
    hidden = refs[8:11], refs[11:14]
    g_own, u_own, d_own, far = refs[14:18]
    for t, here in enumerate(places()):
        rows_x = [rows_of((p[t],), 0, 0, ROWS) for p in pieces]
        rows_y = [rows_of((p[t],), 1, 0, ROWS) for p in pieces]
        for n, own in ((0, g_own), (1, u_own)):
            grad = sum(dot(rows_x[k], hidden[k][1 + n][...], TN) for k in range(2))
            own[here, :] = grad[:, :H]
            far[n, here, :] = grad[:, H:].astype(BF)
        down = sum(dot(hidden[k][0][...], rows_y[k], TN) for k in range(2))
        d_own[:, here] = down[:H]
        far[2, here, :] = down[H:].astype(BF)


def sums_body(g_own, u_own, d_own, far, g_out, u_out, d_out, in_sq, hid_sq):
    ones = jnp.ones((8, H), BF)
    in_sq[...] = jnp.zeros((16, 8, 128), F32)
    for k, (own, out) in enumerate(((g_own, g_out), (u_own, u_out))):
        grad = own[...] + far[k].astype(F32)
        out[...] = grad.astype(BF)
        squares = dot(ones, (grad * grad).astype(BF), NT)
        for b in range(8):
            row = k * 2 + b % 2
            for copy in range(4):
                in_sq[copy * 4 + b // 2, row : row + 1, :] = squares[0:1, b * 128 : (b + 1) * 128]
    total = jnp.zeros((8, H), F32)
    for b in range(4):
        cols = slice(b * H, (b + 1) * H)
        grad = d_own[:, cols] + far[2, cols, :].astype(F32)
        d_out[:, cols] = grad.astype(BF)
        total += dot(ones, (grad * grad).astype(BF), NT)
    hid_sq[...] = total[0:1]


def back_body(order, parts, squares, out):
    norms = jnp.sum(squares[...], axis=0)

    def total(first, count):
        rows = slice(first, first + count)
        added = parts[0, rows, :].astype(F32)
        for k in range(1, 8):
            added += parts[k, rows, :].astype(F32)
        return added

    gates = total(ALL, SRC)
    for b in range(4):
        filled = [total(b * 96, 96), total(ROWS + b * 96, 96), gates[b * 8 : (b + 1) * 8], norms]
        filled = jnp.concatenate(filled, axis=0).astype(BF)
        out[b * 256 : (b + 1) * 256, :] = dot(order[...], filled).astype(BF)


def combine_body(rt, gt, got, out, gate):
    diagonal = iota((T, T), 0) == iota((T, T), 1)

    def put(where, value):
        for x in range(4):
            out[x, where, :] = value.astype(BF)

    def column(row):
        return jnp.sum(jnp.where(diagonal, row, 0.0), axis=1, keepdims=True)

    r0, r1 = (column(rt[k : k + 1, :].astype(F32)).astype(jnp.int32) for k in range(2))
    gates = [column(gt[k : k + 1, :].astype(F32)) for k in range(2)]
    e = iota((T, 128), 1)
    m0, m1 = (e == r0).astype(F32), (e == r1).astype(F32)
    earlier = (iota((T, T), 1) < iota((T, T), 0)).astype(F32).astype(BF)
    before = dot(earlier, (m0 + m1).astype(BF))
    rank0 = jnp.sum(m0 * before, axis=1, keepdims=True).astype(jnp.int32)
    rank1 = jnp.sum(m1 * before, axis=1, keepdims=True).astype(jnp.int32)
    row = iota((T, 1024), 1)
    rows = got[...]
    for half in range(2):
        hit0 = row == r0 * 32 + rank0 + half * 12
        hit1 = row == r1 * 32 + rank1 + half * 12
        pick = jnp.where(hit0 | hit1, 1.0, 0.0).astype(BF)
        put(slice(half * T, (half + 1) * T), dot(pick, rows))
    for k, (r, rank) in enumerate(((r0, rank0), (r1, rank1))):
        both = dot(jnp.where(row == r * 32 + 24, 1.0, 0.0).astype(BF), rows)
        total = jnp.sum(jnp.where(e == rank, both, 0.0), axis=1, keepdims=True)
        share = jnp.where(diagonal, total / gates[k], 0.0)
        gate[k : k + 1, :] = jnp.sum(share, axis=0, keepdims=True)
    n = iota((T, 1024), 0)
    hit = row == (n & 31) * 32 + 25 + ((n >> 5) & 1) * 2 + (n >> 6)
    put(slice(2 * T, 3 * T), dot(jnp.where(hit, 1.0, 0.0).astype(BF), rows))


def final_body(got, token, norms):
    for x in range(4):
        for half in range(2):
            cols = slice((x * 2 + half) * 128, (x * 2 + half + 1) * 128)
            token[:, cols] = got[x, half * T : (half + 1) * T, :]
            first = 2 * T + half * 64
            for kind in range(2):
                rows = got[x, first + kind * 32 : first + kind * 32 + 32, :]
                norms[:, kind, cols] = rows.astype(F32)


SWAP = [(0, 1), (1, 0)]


def turned(x, by):
    return lax.ppermute(x, "tp", [(i, (i + by) % 4) for i in range(4)])


def body(tokens, cotangent, routing, gates, gate_proj, up_proj, down_proj):
    regroup, lane, source, back = tables()
    weights = (gate_proj[0], up_proj[0], down_proj[0])
    sent = call(
        kernel_of(dispatch_body, "dispatch"), shape((1536, 128)),
        routing.T, gates.T, tokens, cotangent,
    )
    others = [lax.ppermute(w, "c", SWAP) for w in weights]
    moved = lax.all_to_all(sent.reshape(SRC, 48, 128), HOMES, 0, 0, tiled=True)
    mine = call(
        kernel_of(regroup_body, "regroup"), shape((1536, 128)), regroup, moved.reshape(1536, 128)
    )
    mine2 = turned(mine, 2)
    near = lax.ppermute(mine, "yp", SWAP)
    mine1, mine3 = turned(mine, 1), turned(mine, -1)
    near2 = lax.ppermute(mine2, "yp", SWAP)
    near1, near3 = turned(near, 1), turned(near, -1)
    pieces, nears = (mine, mine1, mine3, mine2), (near, near1, near3, near2)
    ordered = call(
        kernel_of(prepare_body, "prepare"),
        (shape((D, 2 * H)), shape((D, 2 * H)), shape((2 * H, D))),
        *(w for pair in zip(weights, others) for w in pair),
    )
    hidden = shape((ROWS, 2 * H))
    early, *hidden1 = call(
        kernel_of(first_body, "first", flops=2**31, vmem=VM[0]),
        (shape((4, SENT, 128)), hidden, hidden, hidden), lane, source, *pieces, *ordered,
    )
    rows, *hidden2 = call(
        kernel_of(second_body, "second", flops=2**31, vmem=VM[0]),
        (shape((8, SENT, 128)), hidden, hidden, hidden), lane, source, early, *nears, *ordered,
    )
    parts = lax.all_to_all(rows, GROUP, 0, 0, tiled=True)
    g_own, u_own, d_own, far = call(
        kernel_of(weights_body, "weights", flops=2**31, vmem=VM[1]),
        (shape((D, H), F32), shape((D, H), F32), shape((H, D), F32), shape((3, D, H))),
        *pieces, *nears, *hidden1, *hidden2,
    )
    far = lax.ppermute(far, "c", SWAP)
    gate_grad, up_grad, down_grad, squares, hid_sq = call(
        kernel_of(sums_body, "sums", flops=2**29, vmem=VM[2]),
        (
            shape((D, H)), shape((D, H)), shape((H, D)),
            shape((16, 8, 128), F32), shape((1, H), F32),
        ),
        g_own, u_own, d_own, far,
    )
    squares, parts = lax.optimization_barrier((squares, parts))
    squares = lax.all_to_all(squares, ("c",) + GROUP, 0, 0, tiled=True)
    answer = call(kernel_of(back_body, "back"), shape((1024, 128)), back, parts, squares)
    got = lax.all_to_all(answer.reshape(SRC, 32, 128), HOMES, 0, 0, tiled=True)
    own, gate = call(
        kernel_of(combine_body, "combine"), (shape((4, 384, 128)), shape((2, T), F32)),
        routing.T, gates.T, got.reshape(1024, 128),
    )
    every = lax.all_to_all(own, "tp", 0, 0, tiled=True)
    token, norms = call(
        kernel_of(final_body, "final"), (shape((T, D)), shape((EXPERTS, 2, D), F32)), every
    )
    return (
        token,
        gate.T,
        gate_grad[None],
        up_grad[None],
        down_grad[None],
        norms,
        hid_sq,
    )


def solution(mesh):
    devices = mesh.devices.reshape(8, 4, 2, 2, mesh.shape["tp"])
    split = Mesh(devices, ("z", "yh", "yp", "c", "tp"))
    placed = (
        P(EP, None), P(EP, None), P(EP, None), P(EP, None),
        P(EP, None, "tp"), P(EP, None, "tp"), P(EP, "tp", None),
    )
    return jax.shard_map(
        body,
        mesh=split,
        in_specs=placed,
        out_specs=(
            P(EP, None), P(EP, None), P(EP, None, "tp"), P(EP, None, "tp"), P(EP, "tp", None),
            P(), P(EP, "tp"),
        ),
        check_vma=False,
    )
```

```python
import jax
import jax.numpy as jnp
import numpy as np
from jax import lax
from jax.experimental import pallas as pl
from jax.experimental.pallas import tpu as pltpu
from jax.sharding import Mesh
from jax.sharding import PartitionSpec as P

EP = ("z", "yh", "yp", "c")
HOMES = ("z", "yh")
GROUP = ("yp", "tp")
BF = jnp.bfloat16
F32 = jnp.float32
T, D, H = 128, 1024, 256
EXPERTS, SLOTS, SRC = 32, 12, 32
ROWS = SRC * SLOTS
CH = 192
PART = 2 * CH + 16
TURNS = (0, 3, 1, 2)
NN = (((1,), (0,)), ((), ()))
NT = (((1,), (1,)), ((), ()))
TN = (((0,), (0,)), ((), ()))


def dot(a, b, dims=NN):
    return lax.dot_general(a, b, dims, preferred_element_type=F32)


def iota(shape, dim):
    return lax.broadcasted_iota(jnp.int32, shape, dim)


def kernel(body, name, outs, *args, flops=2**27, vmem=4, spaces=None, out_spaces=None, scratch=(), alias=None):
    vm = pltpu.VMEM
    one = not isinstance(outs, tuple)
    out_spaces = out_spaces or [vm] * (1 if one else len(outs))
    out_specs = tuple(pl.BlockSpec(memory_space=m) for m in out_spaces)
    return pl.pallas_call(
        body,
        out_shape=outs,
        in_specs=[pl.BlockSpec(memory_space=m) for m in (spaces or [vm] * len(args))],
        out_specs=out_specs[0] if one else out_specs,
        scratch_shapes=list(scratch),
        input_output_aliases=alias or {},
        compiler_params=pltpu.CompilerParams(vmem_limit_bytes=vmem * 1024 * 1024),
        cost_estimate=pl.CostEstimate(flops=flops, transcendentals=0, bytes_accessed=2**20),
        name=name,
    )(*args)


def shape(dims, dtype=BF):
    return jax.ShapeDtypeStruct(dims, dtype)


def twelfths(n):
    return (n * 171) >> 11


def ones_where(hit):
    return jnp.where(hit, 1.0, 0.0).astype(BF)


def dispatch_body(rt_in, gt_in, tok_in, cot_in, out, rt, gt, tok, cot, sems):
    cols = pl.ds(pl.multiple_of(lax.axis_index("tp") * H, H), H)
    moves = [
        pltpu.make_async_copy(src, dst, sems.at[n])
        for n, (src, dst) in enumerate(
            ((rt_in, rt), (gt_in, gt), (tok_in.at[:, cols], tok), (cot_in.at[:, cols], cot))
        )
    ]
    for move in moves:
        move.start()
    for move in moves:
        move.wait()
    r0, r1 = rt[0:1, :], rt[1:2, :]
    g0, g1 = gt[0:1, :].astype(F32), gt[1:2, :].astype(F32)
    e = iota((EXPERTS, T), 0)
    m0, m1 = (e == r0).astype(F32), (e == r1).astype(F32)
    earlier = (iota((T, T), 0) < iota((T, T), 1)).astype(F32).astype(BF)
    before = dot((m0 + m1).astype(BF), earlier)
    base0 = r0 * 48 + jnp.sum(m0 * before, axis=0, keepdims=True).astype(jnp.int32)
    base1 = r1 * 48 + jnp.sum(m1 * before, axis=0, keepdims=True).astype(jnp.int32)

    def step(i, carry):
        row = iota((192, T), 0) + i * 192
        total = jnp.zeros((192, 128), F32)
        for half in range(2):
            cols = slice(half * 128, (half + 1) * 128)
            for kind in range(2):
                off = kind * 24 + half * 12
                hit0, hit1 = row == base0 + off, row == base1 + off
                if kind == 0:
                    pick = jnp.where(hit0 | hit1, 1.0, 0.0)
                    total += dot(pick.astype(BF), tok[:, cols])
                else:
                    pick = jnp.where(hit0, g0, jnp.where(hit1, g1, 0.0))
                    total += dot(pick.astype(BF), cot[:, cols])
        out[pl.ds(pl.multiple_of(i * 192, 192), 192), :] = total.astype(BF)
        return carry

    lax.fori_loop(0, 8, step, 0)


def regroup_body(rows, out):
    o, i = iota((192, 192), 0), iota((192, 192), 1)
    k = (o >= 48).astype(jnp.int32) + (o >= 96).astype(jnp.int32) + (o >= 144).astype(jnp.int32)
    rest = o - k * 48
    src = twelfths(rest)
    order = ones_where(i == src * 48 + k * 12 + rest - src * 12)
    for b in range(8):
        moved = dot(order, rows[b * 192 : (b + 1) * 192, :]).astype(BF)
        for k in range(4):
            out[k * ROWS + b * 48 : k * ROWS + (b + 1) * 48, :] = moved[k * 48 : (k + 1) * 48]


def blocks():
    x = lax.axis_index("tp")
    return [lax.rem(x + turn, 4) for turn in TURNS]


def places():
    return [pl.ds(pl.multiple_of(b * H, H), H) for b in blocks()]


def prepare_body(wg, wgo, wu, wuo, wd, wdo, pg, pu, pd):
    for t, here in enumerate(places()):
        there = slice(t * H, (t + 1) * H)
        for mat, mine, other in ((pg, wg, wgo), (pu, wu, wuo)):
            mat[there, :H] = mine[here, :]
            mat[there, H:] = other[here, :]
        pd[:H, there] = wd[:, here]
        pd[H:, there] = wdo[:, here]


def rows_of(pieces, kind, first, count):
    cols = []
    for piece in pieces:
        for half in range(2):
            start = (kind * 2 + half) * ROWS + first
            cols.append(piece[pl.ds(start, count), :])
    return jnp.concatenate(cols, axis=1)


def expert_rows(pieces, pg, pu, pd, out, hidden_out, group, buf, hidden, sems):
    r = iota((CH, 128), 0)
    lane = jnp.where(iota((CH, 128), 1) == r - twelfths(r) * 12, 1.0, 0.0)
    source = ones_where(iota((16, CH), 0) == twelfths(iota((16, CH), 1)))
    moves = []
    for i in range(2):
        kept = slice(i * CH, (i + 1) * CH)
        rows_x = rows_of(pieces, 0, i * CH, CH)
        rows_y = rows_of(pieces, 1, i * CH, CH)
        pre_gate = dot(rows_x, pg[...])
        pre_up = dot(rows_x, pu[...])
        back = dot(rows_y, pd[...], NT)
        s = jax.nn.sigmoid(pre_gate)
        act = pre_gate * s
        prod = act * pre_up
        ggp = (back * pre_up * s * (1.0 + pre_gate * (1.0 - s))).astype(BF)
        gup = (back * act).astype(BF)
        for n, value in enumerate((prod.astype(BF), ggp, gup)):
            hidden[n, kept, :] = value
            to = hidden_out.at[n, kept, :]
            moves.append(pltpu.make_async_copy(hidden.at[n, kept, :], to, sems.at[len(moves)]))
            moves[-1].start()
        part = jnp.sum(back * prod, axis=1, keepdims=True)
        gates = dot(source, (part * lane).astype(BF)).astype(BF)
        grad = (dot(ggp, pg[...], NT) + dot(gup, pu[...], NT)).astype(BF)
        for t, x in enumerate(blocks()):
            for b in range(2):
                cols = slice((t * 2 + b) * 128, (t * 2 + b + 1) * 128)
                buf[i, t, b * CH : (b + 1) * CH, :] = grad[:, cols]
            buf[i, t, 2 * CH : PART, :] = gates
            to = out.at[group * 4 + x, i * PART : (i + 1) * PART, :]
            moves.append(pltpu.make_async_copy(buf.at[i, t], to, sems.at[len(moves)]))
            moves[-1].start()
    for move in moves:
        move.wait()


EXPERT_SCRATCH = (
    pltpu.VMEM((2, 4, 400, 128), BF), pltpu.VMEM((3, 384, 512), BF), pltpu.SemaphoreType.DMA((14,)),
)


def first_body(*refs):
    pieces, (pg, pu, pd), (out, hidden_out) = refs[:4], refs[4:7], refs[7:9]
    half = lax.axis_index("yp")
    expert_rows(pieces, pg, pu, pd, out, hidden_out, half, *refs[9:])


def second_body(early, *refs):
    pieces, (pg, pu, pd), (out, hidden_out) = refs[:4], refs[4:7], refs[7:9]
    half = lax.axis_index("yp")
    expert_rows(pieces, pg, pu, pd, out, hidden_out, 1 - half, *refs[9:])


def weights_body(*refs):
    given, (g_own, u_own, d_own, far), local, sems = refs[:10], refs[10:14], refs[14:24], refs[24]
    moves = [pltpu.make_async_copy(a, b, sems.at[n]) for n, (a, b) in enumerate(zip(given, local))]
    for n in (8, 9, 0, 4, 1, 5, 2, 6, 3, 7):
        moves[n].start()
    pieces, hidden = (local[:4], local[4:8]), local[8:10]
    moves[8].wait()
    moves[9].wait()
    for t, here in enumerate(places()):
        moves[t].wait()
        moves[4 + t].wait()
        rows_x = [rows_of((p[t],), 0, 0, ROWS) for p in pieces]
        rows_y = [rows_of((p[t],), 1, 0, ROWS) for p in pieces]
        for n, own in ((0, g_own), (1, u_own)):
            grad = sum(dot(rows_x[k], hidden[k][1 + n], TN) for k in range(2))
            own[here, :] = grad[:, :H]
            far[n, here, :] = grad[:, H:].astype(BF)
        down = sum(dot(hidden[k][0], rows_y[k], TN) for k in range(2))
        d_own[:, here] = down[:H]
        far[2, here, :] = down[H:].astype(BF)


WEIGHTS_SCRATCH = (
    *[pltpu.VMEM((1536, 128), BF) for _ in range(8)],
    *[pltpu.VMEM((3, 384, 512), BF) for _ in range(2)],
    pltpu.SemaphoreType.DMA((10,)),
)


def sums_body(g_own, u_own, d_own, far, g_out, u_out, d_out, in_sq, hid_sq):
    ones = jnp.ones((8, H), BF)
    in_sq[...] = jnp.zeros((16, 8, 128), F32)
    for k, (own, out) in enumerate(((g_own, g_out), (u_own, u_out))):
        grad = own[...] + far[k].astype(F32)
        out[...] = grad.astype(BF)
        squares = dot(ones, (grad * grad).astype(BF), NT)
        for b in range(8):
            row = k * 2 + b % 2
            for copy in range(4):
                in_sq[copy * 4 + b // 2, row : row + 1, :] = squares[0:1, b * 128 : (b + 1) * 128]
    total = jnp.zeros((8, H), F32)
    for b in range(4):
        cols = slice(b * H, (b + 1) * H)
        grad = d_own[:, cols] + far[2, cols, :].astype(F32)
        d_out[:, cols] = grad.astype(BF)
        total += dot(ones, (grad * grad).astype(BF), NT)
    hid_sq[...] = total[0:1]


def back_body(parts, squares, out):
    norms = jnp.sum(squares[...], axis=0)
    o, i = iota((256, 208), 0), iota((256, 208), 1)
    src, row = o >> 5, o & 31
    late = (row >= 12).astype(jnp.int32)
    at = jnp.where(row < 24, late * 84 + src * 12 + row, jnp.where(row == 24, 192 + src, 175 + row))
    order = ones_where((i == at) & (row < 29))

    def total(first, count):
        rows = slice(first, first + count)
        added = parts[0, rows, :].astype(F32)
        for k in range(1, 8):
            added += parts[k, rows, :].astype(F32)
        return added

    for n in range(2):
        gates = total(n * PART + 2 * CH, 16)
        for b in range(2):
            first = n * PART + b * 96
            filled = [total(first, 96), total(first + CH, 96), gates[b * 8 : (b + 1) * 8], norms]
            filled = jnp.concatenate(filled, axis=0).astype(BF)
            at = (n * 2 + b) * 256
            out[at : at + 256, :] = dot(order, filled).astype(BF)


def combine_body(rt, gt, got, out, gate):
    diagonal = iota((T, T), 0) == iota((T, T), 1)

    def put(where, value):
        for x in range(4):
            out[x, where, :] = value.astype(BF)

    def column(row):
        return jnp.sum(jnp.where(diagonal, row, 0.0), axis=1, keepdims=True)

    r0, r1 = (column(rt[k : k + 1, :].astype(F32)).astype(jnp.int32) for k in range(2))
    gates = [column(gt[k : k + 1, :].astype(F32)) for k in range(2)]
    e = iota((T, 128), 1)
    m0, m1 = (e == r0).astype(F32), (e == r1).astype(F32)
    earlier = (iota((T, T), 1) < iota((T, T), 0)).astype(F32).astype(BF)
    before = dot(earlier, (m0 + m1).astype(BF))
    rank0 = jnp.sum(m0 * before, axis=1, keepdims=True).astype(jnp.int32)
    rank1 = jnp.sum(m1 * before, axis=1, keepdims=True).astype(jnp.int32)
    row = iota((T, 1024), 1)
    rows = got[...]
    for half in range(2):
        hit0 = row == r0 * 32 + rank0 + half * 12
        hit1 = row == r1 * 32 + rank1 + half * 12
        pick = jnp.where(hit0 | hit1, 1.0, 0.0).astype(BF)
        put(slice(half * T, (half + 1) * T), dot(pick, rows))
    for k, (r, rank) in enumerate(((r0, rank0), (r1, rank1))):
        both = dot(jnp.where(row == r * 32 + 24, 1.0, 0.0).astype(BF), rows)
        total = jnp.sum(jnp.where(e == rank, both, 0.0), axis=1, keepdims=True)
        share = jnp.where(diagonal, total / gates[k], 0.0)
        gate[k : k + 1, :] = jnp.sum(share, axis=0, keepdims=True)
    n = iota((T, 1024), 0)
    hit = row == (n & 31) * 32 + 25 + ((n >> 5) & 1) * 2 + (n >> 6)
    put(slice(2 * T, 3 * T), dot(jnp.where(hit, 1.0, 0.0).astype(BF), rows))


def final_body(got, token, norms):
    for x in range(4):
        for half in range(2):
            cols = slice((x * 2 + half) * 128, (x * 2 + half + 1) * 128)
            token[:, cols] = got[x, half * T : (half + 1) * T, :]
            first = 2 * T + half * 64
            for kind in range(2):
                rows = got[x, first + kind * 32 : first + kind * 32 + 32, :]
                norms[:, kind, cols] = rows.astype(F32)


SWAP = [(0, 1), (1, 0)]


def turned(x, by):
    return lax.ppermute(x, "tp", [(i, (i + by) % 4) for i in range(4)])


def body(tokens, cotangent, routing, gates, gate_proj, up_proj, down_proj):
    vm, hbm = pltpu.VMEM, pltpu.HBM
    weights = (gate_proj[0], up_proj[0], down_proj[0])
    sent = kernel(
        dispatch_body, "dispatch", shape((1536, 128)),
        *(pltpu.with_memory_space_constraint(a, hbm) for a in (routing.T, gates.T, tokens, cotangent)),
        spaces=[pltpu.HBM] * 4,
        scratch=(
            pltpu.VMEM((2, T), jnp.int32), pltpu.VMEM((2, T), BF), pltpu.VMEM((T, H), BF),
            pltpu.VMEM((T, H), BF), pltpu.SemaphoreType.DMA((4,)),
        ),
    )
    others = [lax.ppermute(w, "c", SWAP) for w in weights]
    moved = lax.all_to_all(sent.reshape(SRC, 48, 128), HOMES, 0, 0, tiled=True)
    mine = kernel(regroup_body, "regroup", shape((1536, 128)), moved.reshape(1536, 128))
    mine2 = turned(mine, 2)
    near = lax.ppermute(mine, "yp", SWAP)
    mine1, mine3 = turned(mine, 1), turned(mine, -1)
    near2 = lax.ppermute(mine2, "yp", SWAP)
    near1, near3 = turned(near, 1), turned(near, -1)
    pieces, nears = (mine, mine1, mine3, mine2), (near, near1, near3, near2)
    ordered = kernel(
        prepare_body, "prepare", (shape((D, 2 * H)), shape((D, 2 * H)), shape((2 * H, D))),
        *(w for pair in zip(weights, others) for w in pair),
    )
    halves = (hbm((8, 2 * PART, 128), BF), hbm((3, ROWS, 2 * H), BF))
    options = dict(flops=2**31, vmem=8, out_spaces=[hbm, hbm], scratch=EXPERT_SCRATCH)
    early, hidden1 = kernel(first_body, "first", halves, *pieces, *ordered, **options)
    rows, hidden2 = kernel(
        second_body, "second", halves, early, *nears, *ordered,
        spaces=[hbm] + [vm] * 7, alias={0: 0}, **options,
    )
    parts = lax.all_to_all(rows, GROUP, 0, 0, tiled=True)
    given = [pltpu.with_memory_space_constraint(a, hbm) for a in (*pieces, *nears, hidden1, hidden2)]
    g_own, u_own, d_own, far = kernel(
        weights_body, "weights",
        (shape((D, H), F32), shape((D, H), F32), shape((H, D), F32), shape((3, D, H))),
        *given, flops=2**31, vmem=16, spaces=[hbm] * 10, scratch=WEIGHTS_SCRATCH,
    )
    far = lax.ppermute(far, "c", SWAP)
    gate_grad, up_grad, down_grad, squares, hid_sq = kernel(
        sums_body, "sums",
        (
            shape((D, H)), shape((D, H)), shape((H, D)),
            shape((16, 8, 128), F32), shape((1, H), F32),
        ),
        g_own, u_own, d_own, far, flops=2**29, vmem=8,
    )
    squares, parts = lax.optimization_barrier((squares, parts))
    squares = lax.all_to_all(squares, ("c",) + GROUP, 0, 0, tiled=True)
    answer = kernel(back_body, "back", shape((1024, 128)), parts, squares)
    got = lax.all_to_all(answer.reshape(SRC, 32, 128), HOMES, 0, 0, tiled=True)
    own, gate = kernel(
        combine_body, "combine", (shape((4, 384, 128)), shape((2, T), F32)),
        routing.T, gates.T, got.reshape(1024, 128),
    )
    every = lax.all_to_all(own, "tp", 0, 0, tiled=True)
    token, norms = kernel(
        final_body, "final", (shape((T, D)), shape((EXPERTS, 2, D), F32)), every
    )
    return (
        token,
        gate.T,
        gate_grad[None],
        up_grad[None],
        down_grad[None],
        norms,
        hid_sq,
    )


def solution(mesh):
    devices = mesh.devices.reshape(8, 4, 2, 2, mesh.shape["tp"])
    split = Mesh(devices, ("z", "yh", "yp", "c", "tp"))
    placed = (
        P(EP, None), P(EP, None), P(EP, None), P(EP, None),
        P(EP, None, "tp"), P(EP, None, "tp"), P(EP, "tp", None),
    )
    return jax.shard_map(
        body,
        mesh=split,
        in_specs=placed,
        out_specs=(
            P(EP, None), P(EP, None), P(EP, None, "tp"), P(EP, None, "tp"), P(EP, "tp", None),
            P(), P(EP, "tp"),
        ),
        check_vma=False,
    )
```

```python
import jax
import jax.numpy as jnp
from jax import lax
from jax.experimental import pallas as pl
from jax.experimental.pallas import tpu as pltpu
from jax.sharding import Mesh
from jax.sharding import PartitionSpec as P


EP = ("z", "yh", "yp", "c")
HOMES = ("z", "yh")
GROUP = ("yp", "tp")
BF = jnp.bfloat16
F32 = jnp.float32
T, D, H = 128, 1024, 256
EXPERTS, SLOTS, SRC = 32, 12, 32
ROWS = SRC * SLOTS
PART = 2 * ROWS + SRC
TURNS = (0, 3, 1, 2)
NN = (((1,), (0,)), ((), ()))
NT = (((1,), (1,)), ((), ()))
TN = (((0,), (0,)), ((), ()))


def dot(a, b, dims=NN):
    return lax.dot_general(a, b, dims, preferred_element_type=F32)


def iota(shape, dim):
    return lax.broadcasted_iota(jnp.int32, shape, dim)


def kernel(body, outs, *args, flops=2**27, vmem=4, spaces=None, out_spaces=None, scratch=(), alias=None):
    vm = pltpu.VMEM
    one = not isinstance(outs, tuple)
    out_spaces = out_spaces or [vm] * (1 if one else len(outs))
    out_specs = tuple(pl.BlockSpec(memory_space=m) for m in out_spaces)
    return pl.pallas_call(
        body,
        out_shape=outs,
        in_specs=[pl.BlockSpec(memory_space=m) for m in (spaces or [vm] * len(args))],
        out_specs=out_specs[0] if one else out_specs,
        scratch_shapes=list(scratch),
        input_output_aliases=alias or {},
        compiler_params=pltpu.CompilerParams(vmem_limit_bytes=vmem * 1024 * 1024),
        cost_estimate=pl.CostEstimate(flops=flops, transcendentals=0, bytes_accessed=2**20),
    )(*args)


def shape(dims, dtype=BF):
    return jax.ShapeDtypeStruct(dims, dtype)


def twelfths(n):
    return (n * 171) >> 11


def ones_where(hit):
    return jnp.where(hit, 1.0, 0.0).astype(BF)


def dispatch_body(rt_in, gt_in, tok_in, cot_in, out, rt, gt, tok, cot, buf, sems, out_sems):
    cols = pl.ds(pl.multiple_of(lax.axis_index("tp") * H, H), H)
    moves = [
        pltpu.make_async_copy(src, dst, sems.at[n])
        for n, (src, dst) in enumerate(
            ((rt_in, rt), (gt_in, gt), (tok_in.at[:, cols], tok), (cot_in.at[:, cols], cot))
        )
    ]
    for move in moves:
        move.start()
    moves[0].wait()
    moves[1].wait()
    r0, r1 = rt[0:1, :], rt[1:2, :]
    g0, g1 = gt[0:1, :].astype(F32), gt[1:2, :].astype(F32)
    e = iota((EXPERTS, T), 0)
    m0, m1 = (e == r0).astype(F32), (e == r1).astype(F32)
    earlier = (iota((T, T), 0) < iota((T, T), 1)).astype(F32).astype(BF)
    before = dot((m0 + m1).astype(BF), earlier)
    base0 = r0 * 48 + jnp.sum(m0 * before, axis=0, keepdims=True).astype(jnp.int32)
    base1 = r1 * 48 + jnp.sum(m1 * before, axis=0, keepdims=True).astype(jnp.int32)

    moves[2].wait()
    moves[3].wait()

    sends = []
    for i in range(4):
        row = iota((384, T), 0) + i * 384
        total = jnp.zeros((384, 128), F32)
        for half in range(2):
            cols = slice(half * 128, (half + 1) * 128)
            hit0, hit1 = row == base0 + half * 12, row == base1 + half * 12
            total += dot(ones_where(hit0 | hit1), tok[:, cols])
            hit0, hit1 = row == base0 + (24 + half * 12), row == base1 + (24 + half * 12)
            pick = jnp.where(hit0, g0, jnp.where(hit1, g1, 0.0))
            total += dot(pick.astype(BF), cot[:, cols])
        part = slice(i * 384, (i + 1) * 384)
        buf[part, :] = total.astype(BF)
        sends.append(pltpu.make_async_copy(buf.at[part], out.at[part], out_sems.at[i]))
        sends[-1].start()
    for send in sends:
        send.wait()


def regroup_body(rows, out):
    o, i = iota((192, 192), 0), iota((192, 192), 1)
    k = (o >= 48).astype(jnp.int32) + (o >= 96).astype(jnp.int32) + (o >= 144).astype(jnp.int32)
    rest = o - k * 48
    src = twelfths(rest)
    order = ones_where(i == src * 48 + k * 12 + rest - src * 12)
    for b in range(8):
        moved = dot(order, rows[b * 192 : (b + 1) * 192, :]).astype(BF)
        for k in range(4):
            out[k * ROWS + b * 48 : k * ROWS + (b + 1) * 48, :] = moved[k * 48 : (k + 1) * 48]


def blocks():
    x = lax.axis_index("tp")
    return [lax.rem(x + turn, 4) for turn in TURNS]


def places():
    return [pl.ds(pl.multiple_of(b * H, H), H) for b in blocks()]


def prepare_body(wg, wgo, wu, wuo, wd, wdo, pg, pu, pd):
    for t, here in enumerate(places()):
        there = slice(t * H, (t + 1) * H)
        for mat, mine, other in ((pg, wg, wgo), (pu, wu, wuo)):
            mat[there, :H] = mine[here, :]
            mat[there, H:] = other[here, :]
        pd[:H, there] = wd[:, here]
        pd[H:, there] = wdo[:, here]


def rows_of(pieces, kind):
    starts = [(kind * 2 + half) * ROWS for half in range(2)]
    return jnp.concatenate([p[s : s + ROWS, :] for p in pieces for s in starts], axis=1)


def expert_rows(pieces, pg, pu, pd, out, hidden_out, group, buf, hidden, sems):
    r = iota((ROWS, 128), 0)
    lane = jnp.where(iota((ROWS, 128), 1) == r - twelfths(r) * 12, 1.0, 0.0)
    source = ones_where(iota((SRC, ROWS), 0) == twelfths(iota((SRC, ROWS), 1)))
    moves = []
    rows_x = rows_of(pieces, 0)
    rows_y = rows_of(pieces, 1)
    pre_gate = dot(rows_x, pg[...])
    pre_up = dot(rows_x, pu[...])
    back = dot(rows_y, pd[...], NT)
    s = jax.nn.sigmoid(pre_gate)
    act = pre_gate * s
    prod = act * pre_up
    ggp = (back * pre_up * s * (1.0 + pre_gate * (1.0 - s))).astype(BF)
    gup = (back * act).astype(BF)
    for n, value in enumerate((prod.astype(BF), ggp, gup)):
        hidden[n] = value
        moves.append(pltpu.make_async_copy(hidden.at[n], hidden_out.at[n], sems.at[n]))
        moves[-1].start()
    part = jnp.sum(back * prod, axis=1, keepdims=True)
    gates = dot(source, (part * lane).astype(BF)).astype(BF)
    for t, x in enumerate(blocks()):
        there = slice(t * H, (t + 1) * H)
        grad = (dot(ggp, pg[there, :], NT) + dot(gup, pu[there, :], NT)).astype(BF)
        buf[t, :ROWS, :] = grad[:, :128]
        buf[t, ROWS : 2 * ROWS, :] = grad[:, 128:]
        buf[t, 2 * ROWS :, :] = gates
        moves.append(pltpu.make_async_copy(buf.at[t], out.at[group * 4 + x], sems.at[3 + t]))
        moves[-1].start()
    for move in moves:
        move.wait()


EXPERT_SCRATCH = (
    pltpu.VMEM((4, 800, 128), BF), pltpu.VMEM((3, 384, 512), BF), pltpu.SemaphoreType.DMA((7,)),
)


def first_body(*refs):
    pieces, (pg, pu, pd), (out, hidden_out) = refs[:4], refs[4:7], refs[7:9]
    half = lax.axis_index("yp")
    expert_rows(pieces, pg, pu, pd, out, hidden_out, half, *refs[9:])


def second_body(early, *refs):
    pieces, (pg, pu, pd), (out, hidden_out) = refs[:4], refs[4:7], refs[7:9]
    half = lax.axis_index("yp")
    expert_rows(pieces, pg, pu, pd, out, hidden_out, 1 - half, *refs[9:])


def weights_body(*refs):
    given, (g_own, u_own, d_own, far), local, sems = refs[:10], refs[10:14], refs[14:24], refs[24]
    moves = [pltpu.make_async_copy(a, b, sems.at[n]) for n, (a, b) in enumerate(zip(given, local))]
    for n in (8, 9, 0, 4, 1, 5, 2, 6, 3, 7):
        moves[n].start()
    pieces, hidden = (local[:4], local[4:8]), local[8:10]
    moves[8].wait()
    moves[9].wait()
    for t, here in enumerate(places()):
        moves[t].wait()
        moves[4 + t].wait()
        rows_x = [rows_of((p[t],), 0) for p in pieces]
        rows_y = [rows_of((p[t],), 1) for p in pieces]
        for n, own in ((0, g_own), (1, u_own)):
            grad = sum(dot(rows_x[k], hidden[k][1 + n], TN) for k in range(2))
            own[here, :] = grad[:, :H]
            far[n, here, :] = grad[:, H:].astype(BF)
        down = sum(dot(hidden[k][0], rows_y[k], TN) for k in range(2))
        d_own[:, here] = down[:H]
        far[2, here, :] = down[H:].astype(BF)


WEIGHTS_SCRATCH = (
    *[pltpu.VMEM((1536, 128), BF) for _ in range(8)],
    *[pltpu.VMEM((3, 384, 512), BF) for _ in range(2)],
    pltpu.SemaphoreType.DMA((10,)),
)


def sums_body(g_own, u_own, d_own, far, g_out, u_out, d_out, in_sq, hid_sq):
    ones = jnp.ones((8, H), BF)
    in_sq[...] = jnp.zeros((16, 8, 128), F32)
    for k, (own, out) in enumerate(((g_own, g_out), (u_own, u_out))):
        grad = own[...] + far[k].astype(F32)
        out[...] = grad.astype(BF)
        squares = dot(ones, (grad * grad).astype(BF), NT)
        for b in range(8):
            row = k * 2 + b % 2
            for copy in range(4):
                in_sq[copy * 4 + b // 2, row : row + 1, :] = squares[0:1, b * 128 : (b + 1) * 128]
    total = jnp.zeros((8, H), F32)
    for b in range(4):
        cols = slice(b * H, (b + 1) * H)
        grad = d_own[:, cols] + far[2, cols, :].astype(F32)
        d_out[:, cols] = grad.astype(BF)
        total += dot(ones, (grad * grad).astype(BF), NT)
    hid_sq[...] = total[0:1]


def back_body(parts, squares, out):
    norms = jnp.sum(squares[...], axis=0)
    o, i = iota((256, 208), 0), iota((256, 208), 1)
    src, row = o >> 5, o & 31
    late = (row >= 12).astype(jnp.int32)
    at = jnp.where(row < 24, late * 84 + src * 12 + row, jnp.where(row == 24, 192 + src, 175 + row))
    order = ones_where((i == at) & (row < 29))

    def total(first, count):
        rows = slice(first, first + count)
        added = parts[0, rows, :].astype(F32)
        for k in range(1, 8):
            added += parts[k, rows, :].astype(F32)
        return added

    gates = total(2 * ROWS, SRC)
    for b in range(4):
        filled = [total(b * 96, 96), total(ROWS + b * 96, 96), gates[b * 8 : (b + 1) * 8], norms]
        filled = jnp.concatenate(filled, axis=0).astype(BF)
        out[b * 256 : (b + 1) * 256, :] = dot(order, filled).astype(BF)


def combine_body(rt, gt, got, out, gate):
    diagonal = iota((T, T), 0) == iota((T, T), 1)

    def put(where, value):
        for x in range(4):
            out[x, where, :] = value.astype(BF)

    def column(row):
        return jnp.sum(jnp.where(diagonal, row, 0.0), axis=1, keepdims=True)

    r0, r1 = (column(rt[k : k + 1, :].astype(F32)).astype(jnp.int32) for k in range(2))
    gates = [column(gt[k : k + 1, :].astype(F32)) for k in range(2)]
    e = iota((T, 128), 1)
    m0, m1 = (e == r0).astype(F32), (e == r1).astype(F32)
    earlier = (iota((T, T), 1) < iota((T, T), 0)).astype(F32).astype(BF)
    before = dot(earlier, (m0 + m1).astype(BF))
    rank0 = jnp.sum(m0 * before, axis=1, keepdims=True).astype(jnp.int32)
    rank1 = jnp.sum(m1 * before, axis=1, keepdims=True).astype(jnp.int32)
    row = iota((T, 1024), 1)
    rows = got[...]
    for half in range(2):
        hit0 = row == r0 * 32 + rank0 + half * 12
        hit1 = row == r1 * 32 + rank1 + half * 12
        pick = jnp.where(hit0 | hit1, 1.0, 0.0).astype(BF)
        put(slice(half * T, (half + 1) * T), dot(pick, rows))
    for k, (r, rank) in enumerate(((r0, rank0), (r1, rank1))):
        both = dot(jnp.where(row == r * 32 + 24, 1.0, 0.0).astype(BF), rows)
        total = jnp.sum(jnp.where(e == rank, both, 0.0), axis=1, keepdims=True)
        share = jnp.where(diagonal, total / gates[k], 0.0)
        gate[k : k + 1, :] = jnp.sum(share, axis=0, keepdims=True)
    n = iota((T, 1024), 0)
    hit = row == (n & 31) * 32 + 25 + ((n >> 5) & 1) * 2 + (n >> 6)
    put(slice(2 * T, 3 * T), dot(jnp.where(hit, 1.0, 0.0).astype(BF), rows))


def final_body(got, token, norms):
    for x in range(4):
        for half in range(2):
            cols = slice((x * 2 + half) * 128, (x * 2 + half + 1) * 128)
            token[:, cols] = got[x, half * T : (half + 1) * T, :]
            first = 2 * T + half * 64
            for kind in range(2):
                rows = got[x, first + kind * 32 : first + kind * 32 + 32, :]
                norms[:, kind, cols] = rows.astype(F32)


SWAP = [(0, 1), (1, 0)]


def turned(x, by):
    return lax.ppermute(x, "tp", [(i, (i + by) % 4) for i in range(4)])


def body(tokens, cotangent, routing, gates, gate_proj, up_proj, down_proj):
    vm, hbm = pltpu.VMEM, pltpu.HBM
    weights = (gate_proj[0], up_proj[0], down_proj[0])
    sent = kernel(
        dispatch_body, hbm((1536, 128), BF),
        *(pltpu.with_memory_space_constraint(a, hbm) for a in (routing.T, gates.T, tokens, cotangent)),
        spaces=[hbm] * 4, out_spaces=[hbm],
        scratch=(
            pltpu.VMEM((2, T), jnp.int32), pltpu.VMEM((2, T), BF), pltpu.VMEM((T, H), BF),
            pltpu.VMEM((T, H), BF), pltpu.VMEM((1536, 128), BF), pltpu.SemaphoreType.DMA((4,)),
            pltpu.SemaphoreType.DMA((4,)),
        ),
    )
    others = [lax.ppermute(w, "c", SWAP) for w in weights]
    moved = lax.all_to_all(sent.reshape(SRC, 48, 128), HOMES, 0, 0, tiled=True)
    mine = kernel(regroup_body, shape((1536, 128)), moved.reshape(1536, 128))
    mine2 = turned(mine, 2)
    near = lax.ppermute(mine, "yp", SWAP)
    mine1 = turned(mine, 1)
    mine3 = turned(mine, -1)
    near2 = lax.ppermute(mine2, "yp", SWAP)
    near1 = turned(near, 1)
    near3 = turned(near, -1)
    pieces, nears = (mine, mine1, mine3, mine2), (near, near1, near3, near2)
    ordered = kernel(
        prepare_body, (shape((D, 2 * H)), shape((D, 2 * H)), shape((2 * H, D))),
        *(w for pair in zip(weights, others) for w in pair),
    )
    halves = (hbm((8, PART, 128), BF), hbm((3, ROWS, 2 * H), BF))
    options = dict(flops=2**31, vmem=8, out_spaces=[hbm, hbm], scratch=EXPERT_SCRATCH)
    early, hidden1 = kernel(first_body, halves, *pieces, *ordered, **options)
    rows, hidden2 = kernel(
        second_body, halves, early, *nears, *ordered,
        spaces=[hbm] + [vm] * 7, alias={0: 0}, **options,
    )
    parts = lax.all_to_all(rows, GROUP, 0, 0, tiled=True)
    given = [pltpu.with_memory_space_constraint(a, hbm) for a in (*pieces, *nears, hidden1, hidden2)]
    g_own, u_own, d_own, far = kernel(
        weights_body,
        (shape((D, H), F32), shape((D, H), F32), shape((H, D), F32), shape((3, D, H))),
        *given, flops=2**31, vmem=16, spaces=[hbm] * 10, scratch=WEIGHTS_SCRATCH,
    )
    far = lax.ppermute(far, "c", SWAP)
    gate_grad, up_grad, down_grad, squares, hid_sq = kernel(
        sums_body,
        (
            shape((D, H)), shape((D, H)), shape((H, D)),
            shape((16, 8, 128), F32), shape((1, H), F32),
        ),
        g_own, u_own, d_own, far, flops=2**29, vmem=8,
    )
    squares, parts = lax.optimization_barrier((squares, parts))
    squares = lax.all_to_all(squares, ("c",) + GROUP, 0, 0, tiled=True)
    answer = kernel(back_body, shape((1024, 128)), parts, squares)
    got = lax.all_to_all(answer.reshape(SRC, 32, 128), HOMES, 0, 0, tiled=True)
    own, gate = kernel(
        combine_body, (shape((4, 384, 128)), shape((2, T), F32)),
        routing.T, gates.T, got.reshape(1024, 128),
    )
    every = lax.all_to_all(own, "tp", 0, 0, tiled=True)
    token, norms = kernel(final_body, (shape((T, D)), shape((EXPERTS, 2, D), F32)), every)
    return (
        token,
        gate.T,
        gate_grad[None],
        up_grad[None],
        down_grad[None],
        norms,
        hid_sq,
    )


def solution(mesh):
    devices = mesh.devices.reshape(8, 4, 2, 2, mesh.shape["tp"])
    split = Mesh(devices, ("z", "yh", "yp", "c", "tp"))
    placed = (
        P(EP, None), P(EP, None), P(EP, None), P(EP, None),
        P(EP, None, "tp"), P(EP, None, "tp"), P(EP, "tp", None),
    )
    return jax.shard_map(
        body,
        mesh=split,
        in_specs=placed,
        out_specs=(
            P(EP, None), P(EP, None), P(EP, None, "tp"), P(EP, None, "tp"), P(EP, "tp", None),
            P(), P(EP, "tp"),
        ),
        check_vma=False,
    )
```

```python
import jax
import jax.numpy as jnp
from jax import lax
from jax.experimental import pallas as pl
from jax.experimental.pallas import tpu as pltpu
from jax.sharding import Mesh
from jax.sharding import PartitionSpec as P


EP = ("z", "yh", "yp", "c")
HOMES = ("z", "yh")
GROUP = ("yp", "tp")
BF = jnp.bfloat16
F32 = jnp.float32
T, D, H = 128, 1024, 256
EXPERTS, SLOTS, SRC = 32, 12, 32
ROWS = SRC * SLOTS
PART = 2 * ROWS + SRC
TURNS = (0, 3, 1, 2)
NN = (((1,), (0,)), ((), ()))
NT = (((1,), (1,)), ((), ()))
TN = (((0,), (0,)), ((), ()))


def dot(a, b, dims=NN):
    return lax.dot_general(a, b, dims, preferred_element_type=F32)


def iota(shape, dim):
    return lax.broadcasted_iota(jnp.int32, shape, dim)


def kernel(body, outs, *args, flops=2**27, vmem=4, spaces=None, out_spaces=None, scratch=(), alias=None):
    vm = pltpu.VMEM
    one = not isinstance(outs, tuple)
    out_spaces = out_spaces or [vm] * (1 if one else len(outs))
    out_specs = tuple(pl.BlockSpec(memory_space=m) for m in out_spaces)
    return pl.pallas_call(
        body,
        out_shape=outs,
        in_specs=[pl.BlockSpec(memory_space=m) for m in (spaces or [vm] * len(args))],
        out_specs=out_specs[0] if one else out_specs,
        scratch_shapes=list(scratch),
        input_output_aliases=alias or {},
        compiler_params=pltpu.CompilerParams(vmem_limit_bytes=vmem * 1024 * 1024),
        cost_estimate=pl.CostEstimate(flops=flops, transcendentals=0, bytes_accessed=2**20),
    )(*args)


def shape(dims, dtype=BF):
    return jax.ShapeDtypeStruct(dims, dtype)


def twelfths(n):
    return (n * 171) >> 11


def ones_where(hit):
    return jnp.where(hit, 1.0, 0.0).astype(BF)


def dispatch_body(rt_in, gt_in, tok_in, cot_in, out, rt, gt, tok, cot, buf, sems, out_sems):
    cols = pl.ds(pl.multiple_of(lax.axis_index("tp") * H, H), H)
    moves = [
        pltpu.make_async_copy(src, dst, sems.at[n])
        for n, (src, dst) in enumerate(
            ((rt_in, rt), (gt_in, gt), (tok_in.at[:, cols], tok), (cot_in.at[:, cols], cot))
        )
    ]
    for move in moves:
        move.start()
    moves[0].wait()
    moves[1].wait()
    r0, r1 = rt[0:1, :], rt[1:2, :]
    g0, g1 = gt[0:1, :].astype(F32), gt[1:2, :].astype(F32)
    e = iota((EXPERTS, T), 0)
    m0, m1 = (e == r0).astype(F32), (e == r1).astype(F32)
    earlier = (iota((T, T), 0) < iota((T, T), 1)).astype(F32).astype(BF)
    before = dot((m0 + m1).astype(BF), earlier)
    base0 = r0 * 48 + jnp.sum(m0 * before, axis=0, keepdims=True).astype(jnp.int32)
    base1 = r1 * 48 + jnp.sum(m1 * before, axis=0, keepdims=True).astype(jnp.int32)

    moves[2].wait()
    moves[3].wait()

    sends = []
    for i in range(4):
        row = iota((384, T), 0) + i * 384
        total = jnp.zeros((384, 128), F32)
        for half in range(2):
            cols = slice(half * 128, (half + 1) * 128)
            hit0, hit1 = row == base0 + half * 12, row == base1 + half * 12
            total += dot(ones_where(hit0 | hit1), tok[:, cols])
            hit0, hit1 = row == base0 + (24 + half * 12), row == base1 + (24 + half * 12)
            pick = jnp.where(hit0, g0, jnp.where(hit1, g1, 0.0))
            total += dot(pick.astype(BF), cot[:, cols])
        part = slice(i * 384, (i + 1) * 384)
        buf[part, :] = total.astype(BF)
        sends.append(pltpu.make_async_copy(buf.at[part], out.at[part], out_sems.at[i]))
        sends[-1].start()
    for send in sends:
        send.wait()


def regroup_body(rows, out):
    o, i = iota((192, 192), 0), iota((192, 192), 1)
    k = (o >= 48).astype(jnp.int32) + (o >= 96).astype(jnp.int32) + (o >= 144).astype(jnp.int32)
    rest = o - k * 48
    src = twelfths(rest)
    order = ones_where(i == src * 48 + k * 12 + rest - src * 12)
    for b in range(8):
        moved = dot(order, rows[b * 192 : (b + 1) * 192, :]).astype(BF)
        for k in range(4):
            out[k * ROWS + b * 48 : k * ROWS + (b + 1) * 48, :] = moved[k * 48 : (k + 1) * 48]


def blocks():
    x = lax.axis_index("tp")
    return [lax.rem(x + turn, 4) for turn in TURNS]


def places():
    return [pl.ds(pl.multiple_of(b * H, H), H) for b in blocks()]


def prepare_body(wg, wgo, wu, wuo, wd, wdo, pg, pu, pd):
    for t, here in enumerate(places()):
        there = slice(t * H, (t + 1) * H)
        for mat, mine, other in ((pg, wg, wgo), (pu, wu, wuo)):
            mat[there, :H] = mine[here, :]
            mat[there, H:] = other[here, :]
        pd[:H, there] = wd[:, here]
        pd[H:, there] = wdo[:, here]


def rows_of(pieces, kind):
    starts = [(kind * 2 + half) * ROWS for half in range(2)]
    return jnp.concatenate([p[s : s + ROWS, :] for p in pieces for s in starts], axis=1)


def expert_rows(pieces, pg, pu, pd, out, hidden_out, group, buf, hidden, sems):
    r = iota((ROWS, 128), 0)
    lane = jnp.where(iota((ROWS, 128), 1) == r - twelfths(r) * 12, 1.0, 0.0)
    source = ones_where(iota((SRC, ROWS), 0) == twelfths(iota((SRC, ROWS), 1)))
    moves = []
    rows_x = rows_of(pieces, 0)
    rows_y = rows_of(pieces, 1)
    pre_gate = dot(rows_x, pg[...])
    pre_up = dot(rows_x, pu[...])
    back = dot(rows_y, pd[...], NT)
    s = jax.nn.sigmoid(pre_gate)
    act = pre_gate * s
    prod = act * pre_up
    ggp = (back * pre_up * s * (1.0 + pre_gate * (1.0 - s))).astype(BF)
    gup = (back * act).astype(BF)
    for n, value in enumerate((prod.astype(BF), ggp, gup)):
        hidden[n] = value
        moves.append(pltpu.make_async_copy(hidden.at[n], hidden_out.at[n], sems.at[n]))
        moves[-1].start()
    part = jnp.sum(back * prod, axis=1, keepdims=True)
    gates = dot(source, (part * lane).astype(BF)).astype(BF)
    for t, x in enumerate(blocks()):
        there = slice(t * H, (t + 1) * H)
        grad = (dot(ggp, pg[there, :], NT) + dot(gup, pu[there, :], NT)).astype(BF)
        buf[t, :ROWS, :] = grad[:, :128]
        buf[t, ROWS : 2 * ROWS, :] = grad[:, 128:]
        buf[t, 2 * ROWS :, :] = gates
        to = out.at[x, group * PART : (group + 1) * PART]
        moves.append(pltpu.make_async_copy(buf.at[t], to, sems.at[3 + t]))
        moves[-1].start()
    for move in moves:
        move.wait()


EXPERT_SCRATCH = (
    pltpu.VMEM((4, 800, 128), BF), pltpu.VMEM((3, 384, 512), BF), pltpu.SemaphoreType.DMA((7,)),
)


def first_body(*refs):
    expert_rows(refs[:4], *refs[4:9], 0, *refs[9:])


def second_body(early, *refs):
    expert_rows(refs[:4], *refs[4:9], 1, *refs[9:])


def weights_body(*refs):
    given, (g_own, u_own, d_own, far), local, sems = refs[:10], refs[10:14], refs[14:24], refs[24]
    moves = [pltpu.make_async_copy(a, b, sems.at[n]) for n, (a, b) in enumerate(zip(given, local))]
    for n in (8, 9, 0, 4, 1, 5, 2, 6, 3, 7):
        moves[n].start()
    pieces, hidden = (local[:4], local[4:8]), local[8:10]
    moves[8].wait()
    moves[9].wait()
    for t, here in enumerate(places()):
        moves[t].wait()
        moves[4 + t].wait()
        rows_x = [rows_of((p[t],), 0) for p in pieces]
        rows_y = [rows_of((p[t],), 1) for p in pieces]
        for n, own in ((0, g_own), (1, u_own)):
            grad = sum(dot(rows_x[k], hidden[k][1 + n], TN) for k in range(2))
            own[here, :] = grad[:, :H]
            far[n, here, :] = grad[:, H:].astype(BF)
        down = sum(dot(hidden[k][0], rows_y[k], TN) for k in range(2))
        d_own[:, here] = down[:H]
        far[2, here, :] = down[H:].astype(BF)


WEIGHTS_SCRATCH = (
    *[pltpu.VMEM((1536, 128), BF) for _ in range(8)],
    *[pltpu.VMEM((3, 384, 512), BF) for _ in range(2)],
    pltpu.SemaphoreType.DMA((10,)),
)


def sums_body(g_own, u_own, d_own, far, g_out, u_out, d_out, in_sq, hid_sq):
    ones = jnp.ones((8, H), BF)
    in_sq[...] = jnp.zeros((16, 8, 128), F32)
    for k, (own, out) in enumerate(((g_own, g_out), (u_own, u_out))):
        grad = own[...] + far[k].astype(F32)
        out[...] = grad.astype(BF)
        squares = dot(ones, (grad * grad).astype(BF), NT)
        for b in range(8):
            row = k * 2 + b % 2
            for copy in range(4):
                in_sq[copy * 4 + b // 2, row : row + 1, :] = squares[0:1, b * 128 : (b + 1) * 128]
    total = jnp.zeros((8, H), F32)
    for b in range(4):
        cols = slice(b * H, (b + 1) * H)
        grad = d_own[:, cols] + far[2, cols, :].astype(F32)
        d_out[:, cols] = grad.astype(BF)
        total += dot(ones, (grad * grad).astype(BF), NT)
    hid_sq[...] = total[0:1]


def partner_body(parts, out):
    out[...] = sum(parts[k, PART:, :].astype(F32) for k in range(4)).astype(BF)


def back_body(parts, near, squares, out):
    norms = jnp.sum(squares[...], axis=0)
    o, i = iota((256, 208), 0), iota((256, 208), 1)
    src, row = o >> 5, o & 31
    late = (row >= 12).astype(jnp.int32)
    at = jnp.where(row < 24, late * 84 + src * 12 + row, jnp.where(row == 24, 192 + src, 175 + row))
    order = ones_where((i == at) & (row < 29))

    def total(first, count):
        rows = slice(first, first + count)
        return sum((parts[k, rows, :].astype(F32) for k in range(4)), near[rows, :].astype(F32))

    gates = total(2 * ROWS, SRC)
    for b in range(4):
        filled = [total(b * 96, 96), total(ROWS + b * 96, 96), gates[b * 8 : (b + 1) * 8], norms]
        filled = jnp.concatenate(filled, axis=0).astype(BF)
        out[b * 256 : (b + 1) * 256, :] = dot(order, filled).astype(BF)


def combine_body(rt, gt, got, out, gate):
    diagonal = iota((T, T), 0) == iota((T, T), 1)

    def put(where, value):
        for x in range(4):
            out[x, where, :] = value.astype(BF)

    def column(row):
        return jnp.sum(jnp.where(diagonal, row, 0.0), axis=1, keepdims=True)

    r0, r1 = (column(rt[k : k + 1, :].astype(F32)).astype(jnp.int32) for k in range(2))
    gates = [column(gt[k : k + 1, :].astype(F32)) for k in range(2)]
    e = iota((T, 128), 1)
    m0, m1 = (e == r0).astype(F32), (e == r1).astype(F32)
    earlier = (iota((T, T), 1) < iota((T, T), 0)).astype(F32).astype(BF)
    before = dot(earlier, (m0 + m1).astype(BF))
    rank0 = jnp.sum(m0 * before, axis=1, keepdims=True).astype(jnp.int32)
    rank1 = jnp.sum(m1 * before, axis=1, keepdims=True).astype(jnp.int32)
    row = iota((T, 1024), 1)
    rows = got[...]
    for half in range(2):
        hit0 = row == r0 * 32 + rank0 + half * 12
        hit1 = row == r1 * 32 + rank1 + half * 12
        pick = jnp.where(hit0 | hit1, 1.0, 0.0).astype(BF)
        put(slice(half * T, (half + 1) * T), dot(pick, rows))
    for k, (r, rank) in enumerate(((r0, rank0), (r1, rank1))):
        both = dot(jnp.where(row == r * 32 + 24, 1.0, 0.0).astype(BF), rows)
        total = jnp.sum(jnp.where(e == rank, both, 0.0), axis=1, keepdims=True)
        share = jnp.where(diagonal, total / gates[k], 0.0)
        gate[k : k + 1, :] = jnp.sum(share, axis=0, keepdims=True)
    n = iota((T, 1024), 0)
    hit = row == (n & 31) * 32 + 25 + ((n >> 5) & 1) * 2 + (n >> 6)
    put(slice(2 * T, 3 * T), dot(jnp.where(hit, 1.0, 0.0).astype(BF), rows))


def final_body(got, token, norms):
    for x in range(4):
        for half in range(2):
            cols = slice((x * 2 + half) * 128, (x * 2 + half + 1) * 128)
            token[:, cols] = got[x, half * T : (half + 1) * T, :]
            first = 2 * T + half * 64
            for kind in range(2):
                rows = got[x, first + kind * 32 : first + kind * 32 + 32, :]
                norms[:, kind, cols] = rows.astype(F32)


SWAP = [(0, 1), (1, 0)]


def turned(x, by):
    return lax.ppermute(x, "tp", [(i, (i + by) % 4) for i in range(4)])


def body(tokens, cotangent, routing, gates, gate_proj, up_proj, down_proj):
    vm, hbm = pltpu.VMEM, pltpu.HBM
    weights = (gate_proj[0], up_proj[0], down_proj[0])
    sent = kernel(
        dispatch_body, hbm((1536, 128), BF),
        *(pltpu.with_memory_space_constraint(a, hbm) for a in (routing.T, gates.T, tokens, cotangent)),
        spaces=[hbm] * 4, out_spaces=[hbm],
        scratch=(
            pltpu.VMEM((2, T), jnp.int32), pltpu.VMEM((2, T), BF), pltpu.VMEM((T, H), BF),
            pltpu.VMEM((T, H), BF), pltpu.VMEM((1536, 128), BF), pltpu.SemaphoreType.DMA((4,)),
            pltpu.SemaphoreType.DMA((4,)),
        ),
    )
    others = [lax.ppermute(w, "c", SWAP) for w in weights]
    moved = lax.all_to_all(sent.reshape(SRC, 48, 128), HOMES, 0, 0, tiled=True)
    mine = kernel(regroup_body, shape((1536, 128)), moved.reshape(1536, 128))
    mine2 = turned(mine, 2)
    near = lax.ppermute(mine, "yp", SWAP)
    mine1 = turned(mine, 1)
    mine3 = turned(mine, -1)
    near2 = lax.ppermute(mine2, "yp", SWAP)
    near1 = turned(near, 1)
    near3 = turned(near, -1)
    pieces, nears = (mine, mine1, mine3, mine2), (near, near1, near3, near2)
    ordered = kernel(
        prepare_body, (shape((D, 2 * H)), shape((D, 2 * H)), shape((2 * H, D))),
        *(w for pair in zip(weights, others) for w in pair),
    )
    halves = (hbm((4, 2 * PART, 128), BF), hbm((3, ROWS, 2 * H), BF))
    options = dict(flops=2**31, vmem=8, out_spaces=[hbm, hbm], scratch=EXPERT_SCRATCH)
    early, hidden1 = kernel(first_body, halves, *pieces, *ordered, **options)
    rows, hidden2 = kernel(
        second_body, halves, early, *nears, *ordered,
        spaces=[hbm] + [vm] * 7, alias={0: 0}, **options,
    )
    parts = lax.all_to_all(rows, "tp", 0, 0, tiled=True)
    given = [pltpu.with_memory_space_constraint(a, hbm) for a in (*pieces, *nears, hidden1, hidden2)]
    g_own, u_own, d_own, far = kernel(
        weights_body,
        (shape((D, H), F32), shape((D, H), F32), shape((H, D), F32), shape((3, D, H))),
        *given, flops=2**31, vmem=16, spaces=[hbm] * 10, scratch=WEIGHTS_SCRATCH,
    )
    far = lax.ppermute(far, "c", SWAP)
    gate_grad, up_grad, down_grad, squares, hid_sq = kernel(
        sums_body,
        (
            shape((D, H)), shape((D, H)), shape((H, D)),
            shape((16, 8, 128), F32), shape((1, H), F32),
        ),
        g_own, u_own, d_own, far, flops=2**29, vmem=8,
    )
    squares, parts = lax.optimization_barrier((squares, parts))
    squares = lax.all_to_all(squares, ("c",) + GROUP, 0, 0, tiled=True)
    near_sums = kernel(partner_body, shape((PART, 128)), parts)
    near_sums = lax.ppermute(near_sums, "yp", SWAP)
    answer = kernel(back_body, shape((1024, 128)), parts, near_sums, squares)
    got = lax.all_to_all(answer.reshape(SRC, 32, 128), HOMES, 0, 0, tiled=True)
    own, gate = kernel(
        combine_body, (shape((4, 384, 128)), shape((2, T), F32)),
        routing.T, gates.T, got.reshape(1024, 128),
    )
    every = lax.all_to_all(own, "tp", 0, 0, tiled=True)
    token, norms = kernel(final_body, (shape((T, D)), shape((EXPERTS, 2, D), F32)), every)
    return (
        token,
        gate.T,
        gate_grad[None],
        up_grad[None],
        down_grad[None],
        norms,
        hid_sq,
    )


def solution(mesh):
    devices = mesh.devices.reshape(8, 4, 2, 2, mesh.shape["tp"])
    split = Mesh(devices, ("z", "yh", "yp", "c", "tp"))
    placed = (
        P(EP, None), P(EP, None), P(EP, None), P(EP, None),
        P(EP, None, "tp"), P(EP, None, "tp"), P(EP, "tp", None),
    )
    return jax.shard_map(
        body,
        mesh=split,
        in_specs=placed,
        out_specs=(
            P(EP, None), P(EP, None), P(EP, None, "tp"), P(EP, None, "tp"), P(EP, "tp", None),
            P(), P(EP, "tp"),
        ),
        check_vma=False,
    )
```

```python
import jax
import jax.numpy as jnp
from jax import lax
from jax.experimental import pallas as pl
from jax.experimental.pallas import tpu as pltpu
from jax.sharding import Mesh
from jax.sharding import PartitionSpec as P


EP = ("z", "yh", "yp", "c")
HOMES = ("z", "yh")
GROUP = ("yp", "tp")
BF = jnp.bfloat16
F32 = jnp.float32
T, D, H = 128, 1024, 256
EXPERTS, SLOTS, SRC = 32, 12, 32
ROWS = SRC * SLOTS
PART = 2 * ROWS + SRC
TURNS = (0, 3, 1, 2)
NN = (((1,), (0,)), ((), ()))
NT = (((1,), (1,)), ((), ()))
TN = (((0,), (0,)), ((), ()))


def dot(a, b, dims=NN):
    return lax.dot_general(a, b, dims, preferred_element_type=F32)


def iota(shape, dim):
    return lax.broadcasted_iota(jnp.int32, shape, dim)


def kernel(body, outs, *args, flops=2**27, vmem=4, spaces=None, out_spaces=None, scratch=(), alias=None):
    vm = pltpu.VMEM
    one = not isinstance(outs, tuple)
    out_spaces = out_spaces or [vm] * (1 if one else len(outs))
    out_specs = tuple(pl.BlockSpec(memory_space=m) for m in out_spaces)
    return pl.pallas_call(
        body,
        out_shape=outs,
        in_specs=[pl.BlockSpec(memory_space=m) for m in (spaces or [vm] * len(args))],
        out_specs=out_specs[0] if one else out_specs,
        scratch_shapes=list(scratch),
        input_output_aliases=alias or {},
        compiler_params=pltpu.CompilerParams(vmem_limit_bytes=vmem * 1024 * 1024),
        cost_estimate=pl.CostEstimate(flops=flops, transcendentals=0, bytes_accessed=2**20),
    )(*args)


def shape(dims, dtype=BF):
    return jax.ShapeDtypeStruct(dims, dtype)


def twelfths(n):
    return (n * 171) >> 11


def ones_where(hit):
    return jnp.where(hit, 1.0, 0.0).astype(BF)


def dispatch_body(rt_in, gt_in, tok_in, cot_in, out, rt, gt, tok, cot, buf, sems, out_sems):
    cols = pl.ds(pl.multiple_of(lax.axis_index("tp") * H, H), H)
    moves = [
        pltpu.make_async_copy(src, dst, sems.at[n])
        for n, (src, dst) in enumerate(
            ((rt_in, rt), (gt_in, gt), (tok_in.at[:, cols], tok), (cot_in.at[:, cols], cot))
        )
    ]
    for move in moves:
        move.start()
    moves[0].wait()
    moves[1].wait()
    r0, r1 = rt[0:1, :], rt[1:2, :]
    g0, g1 = gt[0:1, :].astype(F32), gt[1:2, :].astype(F32)
    e = iota((EXPERTS, T), 0)
    m0, m1 = (e == r0).astype(F32), (e == r1).astype(F32)
    earlier = (iota((T, T), 0) < iota((T, T), 1)).astype(F32).astype(BF)
    before = dot((m0 + m1).astype(BF), earlier)
    base0 = r0 * 48 + jnp.sum(m0 * before, axis=0, keepdims=True).astype(jnp.int32)
    base1 = r1 * 48 + jnp.sum(m1 * before, axis=0, keepdims=True).astype(jnp.int32)

    moves[2].wait()
    moves[3].wait()

    sends = []
    for i in range(4):
        row = iota((384, T), 0) + i * 384
        total = jnp.zeros((384, 128), F32)
        for half in range(2):
            cols = slice(half * 128, (half + 1) * 128)
            hit0, hit1 = row == base0 + half * 12, row == base1 + half * 12
            total += dot(ones_where(hit0 | hit1), tok[:, cols])
            hit0, hit1 = row == base0 + (24 + half * 12), row == base1 + (24 + half * 12)
            pick = jnp.where(hit0, g0, jnp.where(hit1, g1, 0.0))
            total += dot(pick.astype(BF), cot[:, cols])
        part = slice(i * 384, (i + 1) * 384)
        buf[part, :] = total.astype(BF)
        sends.append(pltpu.make_async_copy(buf.at[part], out.at[part], out_sems.at[i]))
        sends[-1].start()
    for send in sends:
        send.wait()


def regroup_body(rows, out):
    o, i = iota((192, 192), 0), iota((192, 192), 1)
    k = (o >= 48).astype(jnp.int32) + (o >= 96).astype(jnp.int32) + (o >= 144).astype(jnp.int32)
    rest = o - k * 48
    src = twelfths(rest)
    order = ones_where(i == src * 48 + k * 12 + rest - src * 12)
    for b in range(8):
        moved = dot(order, rows[b * 192 : (b + 1) * 192, :]).astype(BF)
        for k in range(4):
            out[k * ROWS + b * 48 : k * ROWS + (b + 1) * 48, :] = moved[k * 48 : (k + 1) * 48]


def blocks():
    x = lax.axis_index("tp")
    return [lax.rem(x + turn, 4) for turn in TURNS]


def places():
    return [pl.ds(pl.multiple_of(b * H, H), H) for b in blocks()]


def prepare_body(wg, wgo, wu, wuo, wd, wdo, pg, pu, pd):
    for t, here in enumerate(places()):
        there = slice(t * H, (t + 1) * H)
        for mat, mine, other in ((pg, wg, wgo), (pu, wu, wuo)):
            mat[there, :H] = mine[here, :]
            mat[there, H:] = other[here, :]
        pd[:H, there] = wd[:, here]
        pd[H:, there] = wdo[:, here]


def rows_of(pieces, kind):
    starts = [(kind * 2 + half) * ROWS for half in range(2)]
    return jnp.concatenate([p[s : s + ROWS, :] for p in pieces for s in starts], axis=1)


def expert_rows(pieces, pg, pu, pd, out, hidden_out, group, buf, hidden, sems):
    r = iota((ROWS, 128), 0)
    lane = jnp.where(iota((ROWS, 128), 1) == r - twelfths(r) * 12, 1.0, 0.0)
    source = ones_where(iota((SRC, ROWS), 0) == twelfths(iota((SRC, ROWS), 1)))
    moves = []
    rows_x = rows_of(pieces, 0)
    rows_y = rows_of(pieces, 1)
    pre_gate = dot(rows_x, pg[...])
    pre_up = dot(rows_x, pu[...])
    back = dot(rows_y, pd[...], NT)
    s = jax.nn.sigmoid(pre_gate)
    act = pre_gate * s
    prod = act * pre_up
    ggp = (back * pre_up * s * (1.0 + pre_gate * (1.0 - s))).astype(BF)
    gup = (back * act).astype(BF)
    for n, value in enumerate((prod.astype(BF), ggp, gup)):
        hidden[n] = value
        moves.append(pltpu.make_async_copy(hidden.at[n], hidden_out.at[n], sems.at[n]))
        moves[-1].start()
    part = jnp.sum(back * prod, axis=1, keepdims=True)
    gates = dot(source, (part * lane).astype(BF)).astype(BF)
    for t, x in enumerate(blocks()):
        there = slice(t * H, (t + 1) * H)
        grad = (dot(ggp, pg[there, :], NT) + dot(gup, pu[there, :], NT)).astype(BF)
        buf[t, :ROWS, :] = grad[:, :128]
        buf[t, ROWS : 2 * ROWS, :] = grad[:, 128:]
        buf[t, 2 * ROWS :, :] = gates
        moves.append(pltpu.make_async_copy(buf.at[t], out.at[group * 4 + x], sems.at[3 + t]))
        moves[-1].start()
    for move in moves:
        move.wait()


EXPERT_SCRATCH = (
    pltpu.VMEM((4, 800, 128), BF), pltpu.VMEM((3, 384, 512), BF), pltpu.SemaphoreType.DMA((7,)),
)


def first_body(*refs):
    pieces, (pg, pu, pd), (out, hidden_out) = refs[:4], refs[4:7], refs[7:9]
    half = lax.axis_index("yp")
    expert_rows(pieces, pg, pu, pd, out, hidden_out, half, *refs[9:])


def second_body(early, *refs):
    pieces, (pg, pu, pd), (out, hidden_out) = refs[:4], refs[4:7], refs[7:9]
    half = lax.axis_index("yp")
    expert_rows(pieces, pg, pu, pd, out, hidden_out, 1 - half, *refs[9:])


def weights_body(*refs):
    given, (g_own, u_own, d_own, far), local, sems = refs[:10], refs[10:14], refs[14:24], refs[24]
    moves = [pltpu.make_async_copy(a, b, sems.at[n]) for n, (a, b) in enumerate(zip(given, local))]
    for n in (8, 9, 0, 4, 1, 5, 2, 6, 3, 7):
        moves[n].start()
    pieces, hidden = (local[:4], local[4:8]), local[8:10]
    moves[8].wait()
    moves[9].wait()
    for t, here in enumerate(places()):
        moves[t].wait()
        moves[4 + t].wait()
        rows_x = [rows_of((p[t],), 0) for p in pieces]
        rows_y = [rows_of((p[t],), 1) for p in pieces]
        for n, own in ((0, g_own), (1, u_own)):
            grad = sum(dot(rows_x[k], hidden[k][1 + n], TN) for k in range(2))
            own[here, :] = grad[:, :H]
            far[n, here, :] = grad[:, H:].astype(BF)
        down = sum(dot(hidden[k][0], rows_y[k], TN) for k in range(2))
        d_own[:, here] = down[:H]
        far[2, here, :] = down[H:].astype(BF)


WEIGHTS_SCRATCH = (
    *[pltpu.VMEM((1536, 128), BF) for _ in range(8)],
    *[pltpu.VMEM((3, 384, 512), BF) for _ in range(2)],
    pltpu.SemaphoreType.DMA((10,)),
)


def sums_body(g_own, u_own, d_own, far, g_out, u_out, d_out, in_sq, hid_sq):
    ones = jnp.ones((8, H), BF)
    in_sq[...] = jnp.zeros((8, 8, 128), F32)
    for k, (own, out) in enumerate(((g_own, g_out), (u_own, u_out))):
        grad = own[...] + far[k].astype(F32)
        out[...] = grad.astype(BF)
        squares = dot(ones, (grad * grad).astype(BF), NT)
        for b in range(8):
            row = k * 2 + b % 2
            for copy in range(2):
                in_sq[copy * 4 + b // 2, row : row + 1, :] = squares[0:1, b * 128 : (b + 1) * 128]
    total = jnp.zeros((8, H), F32)
    for b in range(4):
        cols = slice(b * H, (b + 1) * H)
        grad = d_own[:, cols] + far[2, cols, :].astype(F32)
        d_out[:, cols] = grad.astype(BF)
        total += dot(ones, (grad * grad).astype(BF), NT)
    hid_sq[...] = total[0:1]


def back_body(parts, squares, out):
    norms = jnp.sum(squares[...], axis=0)
    o, i = iota((256, 208), 0), iota((256, 208), 1)
    src, row = o >> 5, o & 31
    late = (row >= 12).astype(jnp.int32)
    at = jnp.where(row < 24, late * 84 + src * 12 + row, jnp.where(row == 24, 192 + src, 175 + row))
    order = ones_where((i == at) & (row < 29))

    def total(first, count):
        rows = slice(first, first + count)
        added = parts[0, rows, :].astype(F32)
        for k in range(1, 8):
            added += parts[k, rows, :].astype(F32)
        return added

    gates = total(2 * ROWS, SRC)
    for b in range(4):
        filled = [total(b * 96, 96), total(ROWS + b * 96, 96), gates[b * 8 : (b + 1) * 8], norms]
        filled = jnp.concatenate(filled, axis=0).astype(BF)
        out[b * 256 : (b + 1) * 256, :] = dot(order, filled).astype(BF)


def combine_body(rt, gt, got, out, gate):
    diagonal = iota((T, T), 0) == iota((T, T), 1)

    def column(row):
        return jnp.sum(jnp.where(diagonal, row, 0.0), axis=1, keepdims=True)

    r0, r1 = (column(rt[k : k + 1, :].astype(F32)).astype(jnp.int32) for k in range(2))
    gates = [column(gt[k : k + 1, :].astype(F32)) for k in range(2)]
    e = iota((T, 128), 1)
    m0, m1 = (e == r0).astype(F32), (e == r1).astype(F32)
    earlier = (iota((T, T), 1) < iota((T, T), 0)).astype(F32).astype(BF)
    before = dot(earlier, (m0 + m1).astype(BF))
    rank0 = jnp.sum(m0 * before, axis=1, keepdims=True).astype(jnp.int32)
    rank1 = jnp.sum(m1 * before, axis=1, keepdims=True).astype(jnp.int32)
    row = iota((T, 1024), 1)
    picks = []
    for half in range(2):
        hit0 = row == r0 * 32 + rank0 + half * 12
        hit1 = row == r1 * 32 + rank1 + half * 12
        picks.append(ones_where(hit0 | hit1))
    n = iota((T, 1024), 0)
    picks.append(ones_where(row == (n & 31) * 32 + 25 + ((n >> 5) & 1) * 2 + (n >> 6)))
    picks += [ones_where(row == r * 32 + 24) for r in (r0, r1)]
    picked = dot(jnp.concatenate(picks, axis=0), got[...])
    for x in range(4):
        out[x] = picked[: 3 * T].astype(BF)
    for k, rank in enumerate((rank0, rank1)):
        both = picked[(3 + k) * T : (4 + k) * T]
        total = jnp.sum(jnp.where(e == rank, both, 0.0), axis=1, keepdims=True)
        share = jnp.where(diagonal, total / gates[k], 0.0)
        gate[k : k + 1, :] = jnp.sum(share, axis=0, keepdims=True)


def final_body(got, token, norms):
    for x in range(4):
        for half in range(2):
            cols = slice((x * 2 + half) * 128, (x * 2 + half + 1) * 128)
            token[:, cols] = got[x, half * T : (half + 1) * T, :]
            first = 2 * T + half * 64
            for kind in range(2):
                rows = got[x, first + kind * 32 : first + kind * 32 + 32, :]
                norms[:, kind, cols] = rows.astype(F32)


SWAP = [(0, 1), (1, 0)]


def turned(x, by):
    return lax.ppermute(x, "tp", [(i, (i + by) % 4) for i in range(4)])


def body(tokens, cotangent, routing, gates, gate_proj, up_proj, down_proj):
    vm, hbm = pltpu.VMEM, pltpu.HBM
    weights = (gate_proj[0], up_proj[0], down_proj[0])
    sent = kernel(
        dispatch_body, hbm((1536, 128), BF),
        *(pltpu.with_memory_space_constraint(a, hbm) for a in (routing.T, gates.T, tokens, cotangent)),
        spaces=[hbm] * 4, out_spaces=[hbm],
        scratch=(
            pltpu.VMEM((2, T), jnp.int32), pltpu.VMEM((2, T), BF), pltpu.VMEM((T, H), BF),
            pltpu.VMEM((T, H), BF), pltpu.VMEM((1536, 128), BF), pltpu.SemaphoreType.DMA((4,)),
            pltpu.SemaphoreType.DMA((4,)),
        ),
    )
    others = [lax.ppermute(w, "c", SWAP) for w in weights]
    moved = lax.all_to_all(sent.reshape(SRC, 48, 128), HOMES, 0, 0, tiled=True)
    mine = kernel(regroup_body, shape((1536, 128)), moved.reshape(1536, 128))
    mine2 = turned(mine, 2)
    near = lax.ppermute(mine, "yp", SWAP)
    mine1 = turned(mine, 1)
    mine3 = turned(mine, -1)
    near2 = lax.ppermute(mine2, "yp", SWAP)
    near1 = turned(near, 1)
    near3 = turned(near, -1)
    pieces, nears = (mine, mine1, mine3, mine2), (near, near1, near3, near2)
    ordered = kernel(
        prepare_body, (shape((D, 2 * H)), shape((D, 2 * H)), shape((2 * H, D))),
        *(w for pair in zip(weights, others) for w in pair),
    )
    halves = (hbm((8, PART, 128), BF), hbm((3, ROWS, 2 * H), BF))
    options = dict(flops=2**31, vmem=8, out_spaces=[hbm, hbm], scratch=EXPERT_SCRATCH)
    early, hidden1 = kernel(first_body, halves, *pieces, *ordered, **options)
    rows, hidden2 = kernel(
        second_body, halves, early, *nears, *ordered,
        spaces=[hbm] + [vm] * 7, alias={0: 0}, **options,
    )
    parts = lax.all_to_all(rows, GROUP, 0, 0, tiled=True)
    given = [pltpu.with_memory_space_constraint(a, hbm) for a in (*pieces, *nears, hidden1, hidden2)]
    g_own, u_own, d_own, far = kernel(
        weights_body,
        (shape((D, H), F32), shape((D, H), F32), shape((H, D), F32), shape((3, D, H))),
        *given, flops=2**31, vmem=16, spaces=[hbm] * 10, scratch=WEIGHTS_SCRATCH,
    )
    far = lax.ppermute(far, "c", SWAP)
    gate_grad, up_grad, down_grad, squares, hid_sq = kernel(
        sums_body,
        (
            shape((D, H)), shape((D, H)), shape((H, D)),
            shape((8, 8, 128), F32), shape((1, H), F32),
        ),
        g_own, u_own, d_own, far, flops=2**29, vmem=8,
    )
    squares = squares + lax.ppermute(squares, "c", SWAP)
    squares, parts = lax.optimization_barrier((squares, parts))
    squares = lax.all_to_all(squares, GROUP, 0, 0, tiled=True)
    answer = kernel(back_body, shape((1024, 128)), parts, squares)
    got = lax.all_to_all(answer.reshape(SRC, 32, 128), HOMES, 0, 0, tiled=True)
    own, gate = kernel(
        combine_body, (shape((4, 384, 128)), shape((2, T), F32)),
        routing.T, gates.T, got.reshape(1024, 128),
    )
    every = lax.all_to_all(own, "tp", 0, 0, tiled=True)
    token, norms = kernel(final_body, (shape((T, D)), shape((EXPERTS, 2, D), F32)), every)
    return (
        token,
        gate.T,
        gate_grad[None],
        up_grad[None],
        down_grad[None],
        norms,
        hid_sq,
    )


def solution(mesh):
    devices = mesh.devices.reshape(8, 4, 2, 2, mesh.shape["tp"])
    split = Mesh(devices, ("z", "yh", "yp", "c", "tp"))
    placed = (
        P(EP, None), P(EP, None), P(EP, None), P(EP, None),
        P(EP, None, "tp"), P(EP, None, "tp"), P(EP, "tp", None),
    )
    return jax.shard_map(
        body,
        mesh=split,
        in_specs=placed,
        out_specs=(
            P(EP, None), P(EP, None), P(EP, None, "tp"), P(EP, None, "tp"), P(EP, "tp", None),
            P(), P(EP, "tp"),
        ),
        check_vma=False,
    )
```
